32 devices in a mesh: grp: 2 (over y), sp: 4 (over z), tp: 4 (over x, core).
Axes of the slice: x: 2, y: 2, z: 4, core: 2. Of those that a mesh axis runs over, the one named last changes fastest.
Arguments:
- tokens: bfloat16 [4096, 4096], P(('grp', 'sp', 'tp')), parts along dimension 0, may hold values from -6 to 6
- norm_gain: float32 [4096], replicated, may hold values from 0.1 to 1.9
- query_diff: bfloat16 [4096, 2048], P('sp', 'tp'), may hold values from -1.25 to 1.25
- key_diff: bfloat16 [4096, 2048], P('sp', 'tp'), may hold values from -1.25 to 1.25
- value_diff: bfloat16 [4096, 2048], P('sp', 'tp'), may hold values from -0.09375 to 0.09375
- lam: float32 [8], P('tp'), may hold values from 0.3 to 0.8
- output_norm_gain: float32 [256], replicated, may hold values from 0.1 to 1.9
- query_win: bfloat16 [4096, 2048], P('sp', 'tp'), may hold values from -1.25 to 1.25
- keyval_win: bfloat16 [4, 4096, 256], P(None, 'sp'), may hold values from -1.25 to 1.25
- sink: float32 [16], P('tp'), may hold values from 4 to 7
- proj_diff: bfloat16 [2048, 4096], P('tp'), may hold values from -0.125 to 0.125
- proj_win: bfloat16 [2048, 4096], P('tp'), may hold values from -0.79296875 to 0.79296875
Outputs:
- mixed: bfloat16 [4096, 4096], P(('grp', 'sp', 'tp')), parts along dimension 0
The draws below stay inside these ranges and needn't reach their ends.
There are 2 independent parts, one for each index of `grp`. The reference program is written for one: setup_inputs(seed, part) draws one part's arguments, and reference() takes and returns one part's arrays. A program takes and returns all parts, laid end to end along the dimension named above; an argument that names none is the same for every part. Nothing has to cross between parts.
All inputs are finite; a program needn't handle non-finite values.
Results may differ from the reference program's by a relative error of at most 0.015.
Values may be sent and summed in bfloat16 or wider, within the bound.
A program may use at most 128 MiB of HBM per device.

```python
import math
import jax
import jax.numpy as jnp
from jax import lax

D = 4096
HEAD = 128
DIFF_HEADS = 8
WIN_HEADS = 16
KV_HEADS = 4
WINDOW = 128
VDIM = 256
SEQ = 2048


def draw_tokens(key, part):
    base = jnp.clip(jax.random.normal(key, (SEQ, D), jnp.float32), -6.0, 6.0)
    return base.astype(jnp.bfloat16)


def diff_pair(key):
    scale = 1.3 * D ** (-0.5)
    width = DIFF_HEADS * 2 * HEAD
    first = jnp.clip(jax.random.normal(jax.random.fold_in(key, 11), (D, width), jnp.float32), -4.0, 4.0) * scale
    second = jnp.clip(jax.random.normal(jax.random.fold_in(key, 12), (D, width), jnp.float32), -4.0, 4.0) * scale
    return (first, second)


def draw_query_diff(key, part):
    return diff_pair(key)[0].astype(jnp.bfloat16)


def draw_key_diff(key, part):
    return diff_pair(key)[1].astype(jnp.bfloat16)


def window_pair(key):
    scale = 1.3 * D ** (-0.5)
    keys = jnp.clip(jax.random.normal(jax.random.fold_in(key, 21), (KV_HEADS, D, HEAD), jnp.float32), -4.0, 4.0) * scale
    values = jnp.clip(jax.random.normal(jax.random.fold_in(key, 22), (KV_HEADS, D, HEAD), jnp.float32), -4.0, 4.0) * D ** (-0.5)
    queries = jnp.clip(jax.random.normal(jax.random.fold_in(key, 23), (D, WIN_HEADS * HEAD), jnp.float32), -4.0, 4.0) * scale
    return (queries, jnp.concatenate([keys, values], axis=2))


def draw_query_win(key, part):
    return window_pair(key)[0].astype(jnp.bfloat16)


def draw_keyval_win(key, part):
    return window_pair(key)[1].astype(jnp.bfloat16)


def shard_levels(rng, dims, split, least, top_value):
    level = 1.0
    for position, parts in split:
        steps = jax.random.uniform(jax.random.fold_in(jax.random.fold_in(rng, 6), position), (parts,), jnp.float32, least / len(split), top_value / len(split))
        level = level * jnp.repeat(jnp.exp(steps), dims[position] // parts).reshape((-1,) + (1,) * (len(dims) - 1 - position))
    return level


def scatter_about(rng, dims, scale, limit, shards=(), kind=jnp.bfloat16):
    values = scale * jax.random.normal(rng, dims, jnp.float32)
    if shards:
        values = values * shard_levels(rng, dims, shards, -0.22, 0.18)
    return jnp.clip(values, -limit, limit).astype(kind)


def setup_inputs(seed: int = 0, part: int = 0) -> dict:
    key_of = jax.random.split(jax.random.key(seed), 13)
    part_splits = jax.random.split(jax.random.fold_in(key_of[12], part), 13)
    return {
        "tokens": draw_tokens(jax.random.fold_in(jax.random.fold_in(key_of[12], part), 71), part),
        "norm_gain": jnp.clip(1.0 + 0.18 * jax.random.normal(key_of[1], (D,), jnp.float32), 0.1, 1.9),
        "query_diff": draw_query_diff(jax.random.fold_in(key_of[12], 71), part),
        "key_diff": draw_key_diff(jax.random.fold_in(key_of[12], 71), part),
        "value_diff": scatter_about(key_of[4], (D, DIFF_HEADS * VDIM), D ** -0.5, 0.09375, ((0, 4), (1, 4))),
        "lam": jnp.clip(0.3 + 0.5 * jax.random.uniform(key_of[5], (DIFF_HEADS,), jnp.float32) ** shard_levels(key_of[5], (DIFF_HEADS,), ((0, 4),), -0.2, 0.2), 0.3, 0.8),
        "output_norm_gain": jnp.clip(1.0 + 0.18 * jax.random.normal(key_of[6], (VDIM,), jnp.float32), 0.1, 1.9),
        "query_win": draw_query_win(jax.random.fold_in(key_of[12], 71), part),
        "keyval_win": draw_keyval_win(jax.random.fold_in(key_of[12], 71), part),
        "sink": jnp.clip(4.0 + 3.0 * jax.random.uniform(key_of[9], (WIN_HEADS,), jnp.float32) ** shard_levels(key_of[9], (WIN_HEADS,), ((0, 4),), -0.2, 0.2), 4.0, 7.0),
        "proj_diff": scatter_about(key_of[10], (DIFF_HEADS * VDIM, D), (DIFF_HEADS * VDIM) ** -0.5, 0.125, ((0, 4),)),
        "proj_win": scatter_about(key_of[11], (WIN_HEADS * HEAD, D), (6 * (WIN_HEADS * HEAD) ** -0.5), 0.79296875, ((0, 4),)),
    }


EPS = 1e-06

def root_mean_square_rows(values, gain):
    return values * lax.rsqrt(lax.optimization_barrier(jnp.mean(values * values, axis=-1, keepdims=True)) + EPS) * gain

def reference(tokens, norm_gain, query_diff, key_diff, value_diff, lam, output_norm_gain, query_win, keyval_win, sink, proj_diff, proj_win):
    seq = tokens.shape[0]
    normed = root_mean_square_rows(tokens.astype(jnp.float32), norm_gain).astype(jnp.bfloat16)

    def project(weight):
        return jnp.dot(normed, weight, preferred_element_type=jnp.float32).astype(jnp.bfloat16)
    q_diff = project(query_diff).reshape(seq, DIFF_HEADS, 2, HEAD)
    k_diff = project(key_diff).reshape(seq, DIFF_HEADS, 2, HEAD)
    v_diff = project(value_diff).reshape(seq, DIFF_HEADS, VDIM)
    q_win = project(query_win).reshape(seq, WIN_HEADS, HEAD)
    kv_win = jnp.stack([project(keyval_win[g]) for g in range(KV_HEADS)], axis=1)
    scale = HEAD ** (-0.5)
    qblock = math.gcd(seq, 512)

    def diff_head(args):
        q_head, k_head, v_head, lambda_head = args

        def one_block(q_rows):
            output_list = []
            for m in range(2):
                scores = jnp.dot(q_rows[:, m], k_head[:, m].T, preferred_element_type=jnp.float32) * scale
                top = lax.optimization_barrier(jnp.max(scores, axis=-1, keepdims=True))
                expo = jnp.exp(scores - top)
                total = lax.optimization_barrier(jnp.sum(expo, axis=-1, keepdims=True))
                output_list.append(jnp.dot(expo.astype(jnp.bfloat16), v_head, preferred_element_type=jnp.float32) / total)
            difference_output = output_list[0] - lambda_head * output_list[1]
            return root_mean_square_rows(difference_output, output_norm_gain).astype(jnp.bfloat16)
        result = lax.map(one_block, q_head.reshape(seq // qblock, qblock, 2, HEAD))
        return result.reshape(seq, VDIM)
    differential_output = lax.map(diff_head, (jnp.transpose(q_diff, (1, 0, 2, 3)), jnp.transpose(k_diff, (1, 0, 2, 3)), jnp.transpose(v_diff, (1, 0, 2)), lam))
    differential_output = jnp.transpose(differential_output, (1, 0, 2)).reshape(seq, DIFF_HEADS * VDIM)
    group = WIN_HEADS // KV_HEADS
    nblocks = seq // WINDOW
    q_blocks = q_win.reshape(nblocks, WINDOW, KV_HEADS, group, HEAD).astype(jnp.float32)
    padded = jnp.pad(kv_win, ((WINDOW, WINDOW), (0, 0), (0, 0))).reshape(nblocks + 2, WINDOW, KV_HEADS, 2 * HEAD)
    band = jnp.concatenate([padded[:-2], padded[1:-1], padded[2:]], axis=1).astype(jnp.float32)
    scores = jnp.einsum('nqgrd,nkgd->ngrqk', q_blocks, band[..., :HEAD]) * scale
    q_index = jnp.arange(WINDOW, dtype=jnp.int32)
    k_index = jnp.arange(3 * WINDOW, dtype=jnp.int32)
    offset = k_index[None, :] - WINDOW - q_index[:, None]
    key_pos = jnp.arange(nblocks, dtype=jnp.int32)[:, None] * WINDOW - WINDOW + k_index[None, :]
    valid = (jnp.abs(offset) <= WINDOW)[None] & ((key_pos >= 0) & (key_pos < seq))[:, None, :]
    scores = jnp.where(valid[:, None, None], scores, -jnp.inf)
    sink_logit = sink.reshape(KV_HEADS, group)[:, :, None, None]
    top = jnp.maximum(lax.optimization_barrier(jnp.max(scores, axis=-1, keepdims=True)), sink_logit)
    expo = jnp.exp(scores - top)
    weights = expo / (lax.optimization_barrier(jnp.sum(expo, axis=-1, keepdims=True)) + jnp.exp(sink_logit - top))
    weights = weights.astype(jnp.bfloat16).astype(jnp.float32)
    y_win = jnp.einsum('ngrqk,nkgd->nqgrd', weights, band[..., HEAD:]).astype(jnp.bfloat16)
    y_win = y_win.reshape(seq, WIN_HEADS * HEAD)
    total = jnp.dot(differential_output, proj_diff, preferred_element_type=jnp.float32)
    total = total + jnp.dot(y_win, proj_win, preferred_element_type=jnp.float32)
    return total.astype(jnp.bfloat16)
```

```python
import functools
import math

import jax
import jax.numpy as jnp
from jax import lax
from jax.experimental import pallas as pl
from jax.experimental.pallas import tpu as pltpu
from jax.sharding import PartitionSpec as P


HEAD = 128
WIN_HEADS = 16
KV_HEADS = 4
WINDOW = 128
VDIM = 256


EPS = 1e-06


def padded_2(x, sides, width):
    for axis, dim in sides:
        devices, length = (lax.axis_size(axis), x.shape[dim])
        up = [(i, (i + 1) % devices) for i in range(devices - 1)]
        down = [(j, i) for i, j in up]
        last = lax.slice_in_dim(x, length - width, length, axis=dim)
        first = lax.slice_in_dim(x, 0, width, axis=dim)
        before = lax.ppermute(last, axis, up)
        after = lax.ppermute(first, axis, down)
        x = jnp.concatenate([before, x, after], axis=dim)
    return x


def root_mean_square_rows(values, gain):
    return values * lax.rsqrt(jnp.mean(values * values, axis=-1, keepdims=True) + EPS) * gain


def shifted(x, axis, by):
    n = lax.axis_size(axis)
    return lax.ppermute(x, axis, [(i, (i + by) % n) for i in range(n)])


def shift_chip(x, by):
    n = lax.axis_size("tp")
    return lax.ppermute(x, "tp", [(i, (i + 2 * by) % n) for i in range(n)])


def swap_core(x):
    n = lax.axis_size("tp")
    return lax.ppermute(x, "tp", [(i, i ^ 1) for i in range(n)])


def gather_tp(x, axis):
    tp = lax.axis_size("tp")
    chips = tp // 2
    me = lax.axis_index("tp")
    mine = [x] + [shift_chip(x, r) for r in range(1, chips)]
    theirs = [swap_core(piece) for piece in mine]
    out = jnp.zeros(x.shape[:axis] + (tp,) + x.shape[axis:], x.dtype)
    for r in range(chips):
        at = (me - 2 * r) % tp
        out = lax.dynamic_update_slice_in_dim(out, jnp.expand_dims(mine[r], axis), at, axis)
        out = lax.dynamic_update_slice_in_dim(out, jnp.expand_dims(theirs[r], axis), at ^ 1, axis)
    return out


def scatter_tp(x):
    tp = lax.axis_size("tp")
    chips = tp // 2
    me = lax.axis_index("tp")
    core, chip = me % 2, me // 2
    x = x.reshape(chips, 2, x.shape[0] // tp, x.shape[1])
    away = lax.dynamic_index_in_dim(x, 1 - core, 1, keepdims=False).astype(jnp.bfloat16)
    keep = lax.dynamic_index_in_dim(x, core, 1, keepdims=False)
    both = keep + swap_core(away).astype(jnp.float32)
    total = lax.dynamic_index_in_dim(both, chip, 0, keepdims=False)
    for r in range(1, chips):
        sent = lax.dynamic_index_in_dim(both, (chip + r) % chips, 0, keepdims=False)
        total = total + shift_chip(sent.astype(jnp.bfloat16), r).astype(jnp.float32)
    return total.astype(jnp.bfloat16)


def diff_kernel(lam_ref, q_ref, k_ref, v_ref, gain_ref, o_ref):
    factor = HEAD ** (-0.5) * math.log2(math.e)
    maps = []
    for m in range(2):
        cols = slice(m * HEAD, (m + 1) * HEAD)
        scores = lax.dot_general(
            q_ref[:, cols], k_ref[:, cols], (((1,), (1,)), ((), ())),
            preferred_element_type=jnp.float32,
        )
        top = jnp.max(scores, axis=-1, keepdims=True)
        expo = jnp.exp2((scores - top) * factor)
        total = jnp.sum(expo, axis=-1, keepdims=True)
        out = jnp.dot(expo.astype(jnp.bfloat16), v_ref[...], preferred_element_type=jnp.float32)
        maps.append(out / total)
    d = maps[0] - lam_ref[pl.program_id(0)] * maps[1]
    d = d * lax.rsqrt(jnp.mean(d * d, axis=-1, keepdims=True) + EPS) * gain_ref[...]
    o_ref[...] = d.astype(jnp.bfloat16)


def diff_attention(q, kv, lam, gain):
    tok, rows, heads = q.shape[0], kv.shape[0], lam.shape[0]
    tile = math.gcd(tok, max(128, 524288 // rows))
    return pl.pallas_call(
        diff_kernel,
        grid=(heads, tok // tile),
        in_specs=[
            pl.BlockSpec(memory_space=pltpu.SMEM),
            pl.BlockSpec((tile, 2 * HEAD), lambda h, i: (i, h)),
            pl.BlockSpec((rows, 2 * HEAD), lambda h, i: (0, h)),
            pl.BlockSpec((rows, VDIM), lambda h, i: (0, heads + h)),
            pl.BlockSpec((1, VDIM), lambda h, i: (0, 0)),
        ],
        out_specs=pl.BlockSpec((tile, VDIM), lambda h, i: (i, h)),
        out_shape=jax.ShapeDtypeStruct((tok, heads * VDIM), jnp.bfloat16),
        cost_estimate=pl.CostEstimate(
            flops=heads * tok * rows * 2 * 2 * (HEAD + VDIM),
            bytes_accessed=2 * (q.size * 2 + kv.size),
            transcendentals=heads * 2 * tok * rows,
        ),
    )(lam, q, kv, kv, gain.reshape(1, VDIM))


def general_body(
    tokens,
    norm_gain,
    query_diff,
    key_diff,
    value_diff,
    lam,
    output_norm_gain,
    query_win,
    keyval_win,
    sink,
    proj_diff,
    proj_win,
):
    bf16, f32 = jnp.bfloat16, jnp.float32
    normed = root_mean_square_rows(tokens.astype(f32), norm_gain).astype(bf16)
    heads_win = sink.shape[0]
    group = WIN_HEADS // KV_HEADS
    n = lax.axis_size("sp")
    me = lax.axis_index("sp")
    parts = lax.axis_size("grp")
    part = lax.axis_index("grp")
    local, width = normed.shape
    depth = width // n
    tok = local * lax.axis_size("tp")

    slabs = normed.reshape(local, n, depth)
    across = jnp.zeros((n, local, depth), bf16)
    own = lax.dynamic_index_in_dim(slabs, me, 1, keepdims=True)
    across = lax.dynamic_update_slice_in_dim(across, jnp.swapaxes(own, 0, 1), me, 0)
    for r in range(1, n):
        sent = lax.dynamic_index_in_dim(slabs, (me + r) % n, 1, keepdims=False)
        got = shifted(sent, "sp", r)
        across = lax.dynamic_update_slice_in_dim(across, got[None], (me - r) % n, 0)

    kv_index = lax.axis_index("tp") * heads_win // group
    kv_local = lax.dynamic_index_in_dim(keyval_win, kv_index, 0, keepdims=False)
    stacked = jnp.concatenate([query_diff, query_win, kv_local], axis=1)
    share = stacked.shape[1] // parts
    half = lax.dynamic_slice_in_dim(stacked, part * share, share, axis=1)
    across, half = lax.optimization_barrier((across, half))

    pieces = [shifted(half, "sp", r) for r in range(1, n)]
    all_rows = gather_tp(across, 1).reshape(n * tok, depth)
    rows_all = gather_tp(normed, 0).reshape(tok, width)
    kv_part = jnp.concatenate(
        [
            jnp.dot(all_rows, key_diff, preferred_element_type=f32).astype(bf16),
            jnp.dot(all_rows, value_diff, preferred_element_type=f32).astype(bf16),
        ],
        axis=1,
    )
    kv = lax.psum_scatter(kv_part, "sp", scatter_dimension=0, tiled=True)
    kv = lax.all_gather(kv, "sp", axis=0, tiled=True)

    own_rows = lax.dynamic_slice_in_dim(rows_all, me * depth, depth, axis=1)
    own_sum = jnp.dot(own_rows, stacked, preferred_element_type=f32)
    sums = [jnp.zeros((tok, share), f32) for _ in range(parts)]
    for r in range(1, n):
        piece = pieces[r - 1]
        rows = lax.dynamic_slice_in_dim(rows_all, (me - r) % n * depth, depth, axis=1)
        for j in range(parts):
            block = piece if j == 0 else shifted(piece, "grp", j)
            sums[j] = sums[j] + jnp.dot(rows, block, preferred_element_type=f32)
    ordered = jnp.stack(sums)
    ordered = jnp.concatenate(
        [
            lax.dynamic_index_in_dim(ordered, (part - b) % parts, 0, keepdims=False)
            for b in range(parts)
        ],
        axis=1,
    )
    projected = (own_sum + ordered).astype(bf16)
    first = query_diff.shape[1]
    second = first + query_win.shape[1]
    q_diff, q_win, kv_win = projected[:, :first], projected[:, first:second], projected[:, second:]
    scale = HEAD ** (-0.5)
    padded = padded_2(kv_win, (("sp", 0),), WINDOW)
    nblocks = tok // WINDOW
    blocks = padded.reshape(nblocks + 2, WINDOW, 2 * HEAD)
    band = jnp.concatenate([blocks[:-2], blocks[1:-1], blocks[2:]], axis=1)
    q_blocks = q_win.reshape(nblocks, WINDOW, heads_win, HEAD)
    scores = (
        jnp.einsum("nqhd,nkd->nhqk", q_blocks, band[..., :HEAD], preferred_element_type=jnp.float32)
        * scale
    )
    q_index = jnp.arange(WINDOW)
    k_index = jnp.arange(3 * WINDOW)
    relative = k_index[None, :] - WINDOW - q_index[:, None]
    first_key = lax.axis_index("sp") * tok - WINDOW
    key_pos = first_key + jnp.arange(nblocks)[:, None] * WINDOW + k_index[None, :]
    inside = (key_pos >= 0) & (key_pos < tok * lax.axis_size("sp"))
    valid = (jnp.abs(relative) <= WINDOW)[None] & inside[:, None, :]
    scores = jnp.where(valid[:, None], scores, -jnp.inf)
    sink_logit = sink[None, :, None, None]
    top_win = jnp.maximum(jnp.max(scores, axis=-1, keepdims=True), sink_logit)
    expo = jnp.exp(scores - top_win)
    weights = expo / (jnp.sum(expo, axis=-1, keepdims=True) + jnp.exp(sink_logit - top_win))
    y_win = jnp.einsum(
        "nhqk,nkd->nqhd",
        weights.astype(jnp.bfloat16),
        band[..., HEAD:],
        preferred_element_type=jnp.float32,
    ).astype(jnp.bfloat16)
    y_win = y_win.reshape(tok, heads_win * HEAD)
    summed = jnp.dot(y_win, proj_win, preferred_element_type=jnp.float32)
    differential_output = diff_attention(q_diff, kv, lam, output_norm_gain)
    summed = summed + jnp.dot(differential_output, proj_diff, preferred_element_type=jnp.float32)
    return scatter_tp(summed)


MESH = pl.DeviceIdType.MESH
CHUNKS = 4
LANES = 128
MATS = 5


def remote(src, dst, send, recv, device):
    return pltpu.make_async_remote_copy(
        src_ref=src, dst_ref=dst, send_sem=send, recv_sem=recv, device_id=device, device_id_type=MESH
    )


def place():
    g, z, t = lax.axis_index("grp"), lax.axis_index("sp"), lax.axis_index("tp")
    x, c = t // 2, t % 2
    return g, z, t, x, c, 2 * (1 - x) + c, 2 * x + 1 - c


def greet(devices):
    barrier = pltpu.get_barrier_semaphore()
    for device in devices:
        pl.semaphore_signal(barrier, inc=1, device_id=device, device_id_type=MESH)
    pl.semaphore_wait(barrier, len(devices))


def project_kernel(
    n, held, tok_ref, gain_ref, qd, qw, kd, vd, kvw, pd, pw, scal_ref,
    res_ref, opd, opw, oscal_ref,
    rows_ref, w_ref, zs, zr, xs, xr, cs, cr, ws, wr, ys, yr, own_sem, rs, rr, ps, pr, scal_s, scal_r,
):
    g, z, t, x, c, t_x, t_c = place()
    local, _ = tok_ref.shape
    part = local // CHUNKS
    depth = qd.shape[0]
    half = depth // 2
    group = WIN_HEADS // KV_HEADS
    mats = (qd, qw, kd, vd, kvw)
    core = (g, z, t_c)

    def block(zz, h, tt):
        return rows_ref.at[zz, h, pl.ds(pl.multiple_of(tt * part, part), part)]

    for h in range(CHUNKS):
        v = tok_ref[h * part:(h + 1) * part, :].astype(jnp.float32)
        v = v * lax.rsqrt(jnp.mean(v * v, axis=-1, keepdims=True) + EPS) * gain_ref[...]
        rows_ref[z, h, pl.ds(pl.multiple_of(t * part, part), part), :] = v.astype(jnp.bfloat16)
    oscal_ref[c] = scal_ref[...]

    greet(
        [(g, lax.rem(z + i // 2, n), 2 * x + (c + i % 2) % 2) for i in range(1, 2 * n)]
        + [(g, z, t_x), (1 - g, z, t)]
    )

    def w_own(zz, yy, m):
        return w_ref.at[pl.ds(pl.multiple_of(zz * depth + yy * half, half), half), m * LANES:(m + 1) * LANES]

    def w_copy(i, cc, m, remote_half):
        dz = c * held + i
        lanes = slice((2 * i + cc) * LANES, (2 * i + cc + 1) * LANES)
        if m == MATS - 1:
            source = kvw.at[(2 * (x * n + dz)) // group]
            lanes = slice(cc * LANES, (cc + 1) * LANES)
        else:
            source = mats[m]
        if remote_half:
            return remote(
                source.at[pl.ds(pl.multiple_of(g * half, half), half), lanes], w_own(z, g, m),
                ws.at[i, cc, m], wr.at[z, m], (g, dz, 2 * x + cc),
            )
        target = w_ref.at[pl.ds(pl.multiple_of(z * depth, depth), depth), m * LANES:(m + 1) * LANES]
        return source.at[:, lanes], target

    def each_weight(act):
        for m in range(MATS):
            for i in range(held):
                for cc in range(2):
                    act(m, i, cc)

    def w_start(m, i, cc):
        dz = c * held + i

        @pl.when(dz != z)
        def _():
            w_copy(i, cc, m, True).start()

    def w_start_own(m, i, cc):
        dz = c * held + i
        source, target = w_copy(i, cc, m, False)

        @pl.when((dz == z) & (cc == c))
        def _():
            pltpu.make_async_copy(source, target, own_sem.at[m]).start()

        @pl.when((dz == z) & (cc != c))
        def _():
            remote(source, target, ws.at[i, cc, m], own_sem.at[m], core).start()

    def w_wait_send(m, i, cc):
        dz = c * held + i
        source, target = w_copy(i, cc, m, False)

        @pl.when(dz != z)
        def _():
            w_copy(i, cc, m, True).wait_send()

        @pl.when((dz == z) & (cc != c))
        def _():
            remote(source, target, ws.at[i, cc, m], own_sem.at[m], core).wait_send()

    def z_copy(way, k, h):
        zz = z - k if way == 0 else z + k
        to = z + 1 if way == 0 else z - 1
        return remote(block(zz, h, t), block(zz, h, t), zs.at[way, k, h], zr.at[way, k + 1, h], (g, to, t))

    def z_wait(way, k, h):
        zz = z - k if way == 0 else z + k
        remote(block(zz, h, t), block(zz, h, t), zs.at[way, k, h], zr.at[way, k, h], core).wait_recv()

    def x_copy(zz, h):
        return remote(block(zz, h, t), block(zz, h, t), xs.at[zz, h], xr.at[zz, h], (g, z, t_x))

    def c_copy(zz, xx, h):
        tt = 2 * xx + c
        return remote(block(zz, h, tt), block(zz, h, tt), cs.at[zz, xx, h], cr.at[zz, xx, h], core)

    def y_copy(zz, m):
        return remote(w_own(zz, g, m), w_own(zz, g, m), ys.at[zz, m], yr.at[zz, m], (1 - g, z, t))

    each_weight(w_start)
    for h in range(CHUNKS):
        @pl.when(z < n - 1)
        def _(h=h):
            z_copy(0, 0, h).start()

        @pl.when(z > 0)
        def _(h=h):
            z_copy(1, 0, h).start()

        x_copy(z, h).start()
        c_copy(z, x, h).start()
    scal_copy = remote(scal_ref, oscal_ref.at[c], scal_s, scal_r, core)
    scal_copy.start()
    each_weight(w_start_own)
    proj_copies = [remote(pd, opd, ps.at[0], pr.at[0], core), remote(pw, opw, ps.at[1], pr.at[1], core)]
    for copy in proj_copies:
        copy.start()

    def sides(k, act):
        @pl.when(z - k >= 0)
        def _():
            act(z - k, 0)

        @pl.when((z + k < n) & (k > 0))
        def _():
            act(z + k, 1)

    for d in range(1, n):
        def forward(zz, way):
            def one(m):
                remote(w_own(zz, g, m), w_own(zz, g, m), ys.at[zz, m], wr.at[zz, m], core).wait_recv()
                y_copy(zz, m).start()

            for m in range(MATS):
                one(m)

        sides(d, forward)

    def stage_a(e):
        k, h = e // CHUNKS, e % CHUNKS

        def act(zz, way):
            z_wait(way, k, h)

            @pl.when(z < n - 1 if way == 0 else z > 0)
            def _():
                z_copy(way, k, h).start()

            x_copy(zz, h).start()
            c_copy(zz, x, h).start()

        sides(k, act)

    def stage_b(e):
        k, h = e // CHUNKS, e % CHUNKS

        def act(zz, way):
            x_copy(zz, h).wait_recv()
            c_copy(zz, 1 - x, h).start()

        sides(k, act)

    def stage_c(e, carry):
        k, h = e // CHUNKS, e % CHUNKS

        def act(zz, way):
            for xx in range(2):
                c_copy(zz, xx, h).wait_recv()
            res_ref[c, zz, h] = jnp.dot(
                rows_ref[zz, h], w_ref[...], preferred_element_type=jnp.float32
            ).astype(jnp.bfloat16)

        sides(k, act)
        return carry

    def r_copies(zz, h):
        copies = [remote(
            res_ref.at[c, zz, h, :, 2 * LANES:], res_ref.at[c, zz, h, :, 2 * LANES:],
            rs.at[zz, h, 0], rr.at[zz, h, 0], core,
        )]
        for xx in range(2):
            at = pl.ds(pl.multiple_of((2 * xx + 1 - c) * part, part), part)
            copies.append(remote(
                res_ref.at[c, zz, h, at, :2 * LANES], res_ref.at[c, zz, h, at, :2 * LANES],
                rs.at[zz, h, 1 + xx], rr.at[zz, h, 1 + xx], core,
            ))
        return copies

    def stage_d(e, carry):
        k, h = e // CHUNKS, e % CHUNKS

        def act(zz, way):
            for copy in r_copies(zz, h):
                copy.start()

        sides(k, act)
        return carry

    for e in range(CHUNKS - 1):
        stage_b(e)

    last = n * CHUNKS

    def upto(e):
        return jnp.maximum(jnp.minimum(2 * (e - 2 * CHUNKS + 1), e - 1), 0)

    def weights_ready():
        for m in range(MATS):
            source, target = w_copy(0, 0, m, False)
            pltpu.make_async_copy(source, target, own_sem.at[m]).wait()
        for d in range(1, n):
            def arrived(zz, way):
                for m in range(MATS):
                    remote(w_own(zz, 1 - g, m), w_own(zz, 1 - g, m), ys.at[zz, m], yr.at[zz, m], core).wait_recv()

            sides(d, arrived)

    def step(e, carry):
        @pl.when(e < last)
        def _():
            stage_a(e)

        @pl.when(e < last + 1)
        def _():
            stage_b(e - 1)

        pl.when(e == 2 * CHUNKS)(weights_ready)
        lax.fori_loop(upto(e - 2), upto(e - 1), stage_d, 0)
        lax.fori_loop(upto(e - 1), upto(e), stage_c, 0)
        return carry

    lax.fori_loop(CHUNKS, last + 2, step, 0)
    for copy in proj_copies + [scal_copy]:
        copy.wait()
    each_weight(w_wait_send)
    lax.fori_loop(upto(last), upto(last + 1), stage_d, 0)

    def drain(e, carry):
        k, h = e // CHUNKS, e % CHUNKS

        def act(zz, way):
            @pl.when(z < n - 1 if way == 0 else z > 0)
            def _():
                z_copy(way, k, h).wait_send()

            x_copy(zz, h).wait_send()
            for xx in range(2):
                c_copy(zz, xx, h).wait_send()
            for copy in r_copies(zz, h):
                copy.wait()

        sides(k, act)

        @pl.when((k == 0) & (z > 0))
        def _():
            z_copy(1, 0, h).wait_send()

        return carry

    lax.fori_loop(0, last, drain, 0)
    for d in range(1, n):
        def sent(zz, way):
            for m in range(MATS):
                y_copy(zz, m).wait_send()

        sides(d, sent)


def project(n, tokens, norm_gain, query_diff, query_win, key_diff, value_diff, keyval_win, proj_diff, proj_win, scal):
    local, width = tokens.shape
    held = n // 2
    dma = pltpu.SemaphoreType.DMA
    whole = pl.BlockSpec(memory_space=pltpu.VMEM)
    far = pl.BlockSpec(memory_space=pl.ANY)
    cols = MATS * LANES
    tok = 4 * local * n
    return pl.pallas_call(
        functools.partial(project_kernel, n, held),
        in_specs=[whole, whole] + [far] * 7 + [whole],
        out_specs=[whole, far, far, whole],
        out_shape=[
            jax.ShapeDtypeStruct((2, n, CHUNKS, 4 * local // CHUNKS, cols), jnp.bfloat16),
            jax.ShapeDtypeStruct(proj_diff.shape, proj_diff.dtype),
            jax.ShapeDtypeStruct(proj_win.shape, proj_win.dtype),
            jax.ShapeDtypeStruct((2,) + scal.shape, scal.dtype),
        ],
        scratch_shapes=[
            pltpu.VMEM((n, CHUNKS, 4 * local // CHUNKS, width), jnp.bfloat16),
            pltpu.VMEM((width, cols), jnp.bfloat16),
            dma((2, n, CHUNKS)), dma((2, n + 1, CHUNKS)),
            dma((n, CHUNKS)), dma((n, CHUNKS)),
            dma((n, 2, CHUNKS)), dma((n, 2, CHUNKS)),
            dma((held, 2, MATS)), dma((n, MATS)),
            dma((n, MATS)), dma((n, MATS)), dma((MATS,)),
            dma((n, CHUNKS, 3)), dma((n, CHUNKS, 3)),
            dma((2,)), dma((2,)), dma, dma,
        ],
        compiler_params=pltpu.CompilerParams(
            collective_id=0, has_side_effects=True, vmem_limit_bytes=52 << 20
        ),
        cost_estimate=pl.CostEstimate(
            flops=2 * tok * width * cols, bytes_accessed=2 * width * (tok + cols), transcendentals=0
        ),
    )(tokens, norm_gain.reshape(1, width), query_diff, query_win, key_diff, value_diff, keyval_win, proj_diff, proj_win, scal)


def attend_kernel(n, scal_ref, res_ref, gain_ref, y_ref, v_ref):
    z, t = lax.axis_index("sp"), lax.axis_index("tp")
    c = t % 2
    zz = pl.program_id(0)
    chunks, quad, _ = res_ref.shape[2:]
    part = quad // 4
    local = part * chunks
    rows = n * chunks * quad
    factor = HEAD ** (-0.5) * math.log2(math.e)
    f32, bf16 = jnp.float32, jnp.bfloat16

    @pl.when(zz == 0)
    def _():
        for i in range(2):
            v_ref[:, i * LANES:(i + 1) * LANES] = res_ref[i, :, :, :, 3 * LANES:4 * LANES].reshape(rows, LANES)

    def own(i, xx, m):
        at = pl.ds(pl.multiple_of((2 * xx + c) * part, part), part)
        return res_ref[i, zz, :, at, m * LANES:(m + 1) * LANES].reshape(local, LANES)

    maps = []
    for m in range(2):
        q = jnp.concatenate([own(m, xx, 0) for xx in range(2)], axis=0)
        keys = res_ref[m, :, :, :, 2 * LANES:3 * LANES].reshape(rows, LANES)
        scores = lax.dot_general(q, keys, (((1,), (1,)), ((), ())), preferred_element_type=f32)
        top = jnp.max(scores, axis=-1, keepdims=True)
        expo = jnp.exp2((scores - top) * factor)
        total = jnp.sum(expo, axis=-1, keepdims=True)
        out = jnp.dot(expo.astype(bf16), v_ref[...], preferred_element_type=f32)
        maps.append(out / total)
    lam = scal_ref[z // (n // 2), 0, z % (n // 2)]
    d = maps[0] - lam * maps[1]
    d = d * lax.rsqrt(jnp.mean(d * d, axis=-1, keepdims=True) + EPS) * gain_ref[...]
    y_ref[0, :, :, :VDIM] = d.astype(bf16).reshape(2, local, VDIM)

    held = n // 2
    r_index = lax.broadcasted_iota(jnp.int32, (2 * local, 3 * local), 0) % local
    k_index = lax.broadcasted_iota(jnp.int32, (2 * local, 3 * local), 1)
    near = jnp.abs(k_index - local - r_index) <= WINDOW
    first = lax.broadcasted_iota(jnp.int32, (2 * local, 1), 0) < local
    sinks = [scal_ref[z // held, 1, 2 * (z % held) + i] for i in range(2)]
    sink = jnp.where(first, sinks[0], sinks[1])
    for xx in range(2):
        b = 4 * zz + 2 * xx + c

        def banded(i):
            pieces = []
            for s in (-1, 0, 1):
                o = jnp.clip(b + s, 0, 4 * n - 1)
                at = pl.ds(pl.multiple_of(o % 4 * part, part), part)
                pieces.append(res_ref[i, o // 4, :, at, 4 * LANES:5 * LANES].reshape(local, LANES))
            return jnp.concatenate(pieces, axis=0)

        q = jnp.concatenate([own(i, xx, 1) for i in range(2)], axis=0)
        scores = lax.dot_general(
            q, banded(0), (((1,), (1,)), ((), ())), preferred_element_type=f32
        ) * HEAD ** (-0.5)
        spot = (b - 1) * local + k_index
        valid = near & (spot >= 0) & (spot < rows)
        scores = jnp.where(valid, scores, -jnp.inf)
        top = jnp.maximum(jnp.max(scores, axis=-1, keepdims=True), sink)
        expo = jnp.exp(scores - top)
        weights = expo / (jnp.sum(expo, axis=-1, keepdims=True) + jnp.exp(sink - top))
        out = jnp.dot(weights.astype(bf16), banded(1), preferred_element_type=f32).astype(bf16)
        for i in range(2):
            y_ref[0, xx, :, VDIM + i * LANES:VDIM + (i + 1) * LANES] = out[i * local:(i + 1) * local]


def attend(n, scal, res, gain):
    chunks, quad, _ = res.shape[2:]
    local = quad * chunks // 4
    rows = n * chunks * quad
    feats = VDIM + 2 * HEAD
    return pl.pallas_call(
        functools.partial(attend_kernel, n),
        grid=(n,),
        in_specs=[
            pl.BlockSpec(memory_space=pltpu.SMEM),
            pl.BlockSpec(memory_space=pltpu.VMEM),
            pl.BlockSpec(memory_space=pltpu.VMEM),
        ],
        out_specs=pl.BlockSpec((1, 2, local, feats), lambda i: (i, 0, 0, 0)),
        out_shape=jax.ShapeDtypeStruct((n, 2, local, feats), jnp.bfloat16),
        scratch_shapes=[pltpu.VMEM((rows, VDIM), jnp.bfloat16)],
        cost_estimate=pl.CostEstimate(
            flops=rows * rows * 2 * (HEAD + VDIM), bytes_accessed=2 * res.size, transcendentals=rows * rows
        ),
    )(scal, res, gain.reshape(1, VDIM))


def finish_kernel(
    n, y_ref, pd, pw, opd, opw, out_ref,
    got_ref, p_ref, mine_ref, away_ref, theirs_ref, ys, yr, load, ds, dr,
):
    g, z, t, x, c, t_x, _ = place()
    held = n // 2
    local, width = out_ref.shape
    steps = mine_ref.shape[0]
    wide = width // steps
    f32, bf16 = jnp.float32, jnp.bfloat16

    loads = []
    for i in range(held):
        for far, at, a, b in ((0, c, pd, pw), (1, 1 - c, opd, opw)):
            for j, ref in enumerate((a, b)):
                loads.append(pltpu.make_async_copy(
                    ref.at[i * VDIM:(i + 1) * VDIM], p_ref.at[at * held + i, j * VDIM:(j + 1) * VDIM],
                    load.at[i, far, j],
                ))
    for copy in loads:
        copy.start()

    greet([(g, lax.rem(z + i, n), t) for i in range(1, n)] + [(g, z, t_x)])

    def y_copy(zz, xx):
        return remote(y_ref.at[zz, xx], got_ref.at[z, xx], ys.at[zz, xx], yr.at[z, xx], (g, zz, t))

    def y_wait(zz, xx):
        return remote(got_ref.at[zz, xx], got_ref.at[zz, xx], ys.at[zz, xx], yr.at[zz, xx], (g, z, t_x))

    def others(act):
        for d in range(n - 1, 0, -1):
            pl.when(z - d >= 0)(functools.partial(act, z - d))
            pl.when(z + d < n)(functools.partial(act, z + d))

    for xx in (1 - x, x):
        others(lambda zz: y_copy(zz, xx).start())
    got_ref[z] = y_ref[z]
    for copy in loads:
        copy.wait()

    def product(j, xx):
        total = jnp.zeros((local, wide), f32)
        at = pl.ds(pl.multiple_of(j * wide, wide), wide)
        for zz in range(n):
            total = total + jnp.dot(got_ref[zz, xx], p_ref[zz, :, at], preferred_element_type=f32)
        return total

    def d_copy(j):
        return remote(away_ref.at[j], theirs_ref.at[j], ds.at[j], dr.at[j], (g, z, t_x))

    others(lambda zz: y_wait(zz, 1 - x).wait_recv())

    def send(j, carry):
        value = product(j, 1 - x).astype(bf16)

        @pl.when(j > 0)
        def _():
            d_copy(j - 1).start()

        away_ref[j] = value
        return carry

    lax.fori_loop(0, steps, send, 0)
    others(lambda zz: y_wait(zz, x).wait_recv())
    d_copy(steps - 1).start()

    def keep(j, carry):
        mine_ref[j] = product(j, x)
        return carry

    lax.fori_loop(0, steps, keep, 0)
    for j in range(steps):
        d_copy(j).wait_recv()
        out_ref[:, j * wide:(j + 1) * wide] = (mine_ref[j] + theirs_ref[j].astype(f32)).astype(bf16)
    for j in range(steps):
        d_copy(j).wait_send()
    for xx in (1 - x, x):
        others(lambda zz: y_copy(zz, xx).wait_send())


def finish(n, y, proj_diff, proj_win, other_diff, other_win):
    local, feats = y.shape[2:]
    width = proj_diff.shape[1]
    steps = 8
    dma = pltpu.SemaphoreType.DMA
    whole = pl.BlockSpec(memory_space=pltpu.VMEM)
    far = pl.BlockSpec(memory_space=pl.ANY)
    return pl.pallas_call(
        functools.partial(finish_kernel, n),
        in_specs=[whole] + [far] * 4,
        out_specs=whole,
        out_shape=jax.ShapeDtypeStruct((local, width), jnp.bfloat16),
        scratch_shapes=[
            pltpu.VMEM(y.shape, jnp.bfloat16),
            pltpu.VMEM((n, feats, width), jnp.bfloat16),
            pltpu.VMEM((steps, local, width // steps), jnp.float32),
            pltpu.VMEM((steps, local, width // steps), jnp.bfloat16),
            pltpu.VMEM((steps, local, width // steps), jnp.bfloat16),
            dma((n, 2)), dma((n, 2)), dma((n // 2, 2, 2)), dma((steps,)), dma((steps,)),
        ],
        compiler_params=pltpu.CompilerParams(
            collective_id=1, has_side_effects=True, vmem_limit_bytes=52 << 20
        ),
        cost_estimate=pl.CostEstimate(
            flops=2 * 2 * local * n * feats * width, bytes_accessed=2 * n * feats * width, transcendentals=0
        ),
    )(y, proj_diff, proj_win, other_diff, other_win)


def split_body(
    tokens, norm_gain, query_diff, key_diff, value_diff, lam, output_norm_gain,
    query_win, keyval_win, sink, proj_diff, proj_win,
):
    n = lax.axis_size("sp")
    scal = jnp.stack([jnp.pad(lam, (0, LANES - lam.shape[0])), jnp.pad(sink, (0, LANES - sink.shape[0]))])
    scal = jnp.pad(scal, ((0, 6), (0, 0)))
    res, other_diff, other_win, both = project(
        n, tokens, norm_gain, query_diff, query_win, key_diff, value_diff, keyval_win, proj_diff, proj_win, scal
    )
    y = attend(n, both, res, output_norm_gain)
    return finish(n, y, proj_diff, proj_win, other_diff, other_win)


def splits(mesh, tokens, query_diff, query_win, lam, sink):
    parts, n, tp = (mesh.shape[a] for a in ("grp", "sp", "tp"))
    return (
        parts == 2 and tp == 4 and n % 2 == 0
        and lam.shape[0] == 2 * n and sink.shape[0] == 2 * lam.shape[0]
        and tokens.shape[0] == parts * n * tp * WINDOW
        and query_diff.shape[1] == lam.shape[0] * 2 * HEAD and VDIM == 2 * HEAD
        and query_win.shape[1] == sink.shape[0] * HEAD and HEAD == LANES
    )


def solution(mesh):
    placed = (
        P(("grp", "sp", "tp"), None),
        P(),
        P("sp", "tp"),
        P("sp", "tp"),
        P("sp", "tp"),
        P("tp"),
        P(),
        P("sp", "tp"),
        P(None, "sp", None),
        P("tp"),
        P("tp", None),
        P("tp", None),
    )

    def build(body):
        return jax.shard_map(
            body, mesh=mesh, in_specs=placed, out_specs=P(("grp", "sp", "tp"), None), check_vma=False
        )

    general = build(general_body)

    def step(*args):
        tokens, query_diff, lam, query_win, sink = (args[i] for i in (0, 2, 5, 7, 9))
        if splits(mesh, tokens, query_diff, query_win, lam, sink):
            return build(split_body)(*args)
        return general(*args)

    return step
```

```python
import functools
import math

import jax
import jax.numpy as jnp
from jax import lax
from jax.experimental import pallas as pl
from jax.experimental.pallas import tpu as pltpu
from jax.sharding import PartitionSpec as P


HEAD = 128
WIN_HEADS = 16
KV_HEADS = 4
WINDOW = 128
VDIM = 256


EPS = 1e-06


def padded_2(x, sides, width):
    for axis, dim in sides:
        devices, length = (lax.axis_size(axis), x.shape[dim])
        up = [(i, (i + 1) % devices) for i in range(devices - 1)]
        down = [(j, i) for i, j in up]
        last = lax.slice_in_dim(x, length - width, length, axis=dim)
        first = lax.slice_in_dim(x, 0, width, axis=dim)
        before = lax.ppermute(last, axis, up)
        after = lax.ppermute(first, axis, down)
        x = jnp.concatenate([before, x, after], axis=dim)
    return x


def root_mean_square_rows(values, gain):
    return values * lax.rsqrt(jnp.mean(values * values, axis=-1, keepdims=True) + EPS) * gain


def shifted(x, axis, by):
    n = lax.axis_size(axis)
    return lax.ppermute(x, axis, [(i, (i + by) % n) for i in range(n)])


def shift_chip(x, by):
    n = lax.axis_size("tp")
    return lax.ppermute(x, "tp", [(i, (i + 2 * by) % n) for i in range(n)])


def swap_core(x):
    n = lax.axis_size("tp")
    return lax.ppermute(x, "tp", [(i, i ^ 1) for i in range(n)])


def gather_tp(x, axis):
    tp = lax.axis_size("tp")
    chips = tp // 2
    me = lax.axis_index("tp")
    mine = [x] + [shift_chip(x, r) for r in range(1, chips)]
    theirs = [swap_core(piece) for piece in mine]
    out = jnp.zeros(x.shape[:axis] + (tp,) + x.shape[axis:], x.dtype)
    for r in range(chips):
        at = (me - 2 * r) % tp
        out = lax.dynamic_update_slice_in_dim(out, jnp.expand_dims(mine[r], axis), at, axis)
        out = lax.dynamic_update_slice_in_dim(out, jnp.expand_dims(theirs[r], axis), at ^ 1, axis)
    return out


def scatter_tp(x):
    tp = lax.axis_size("tp")
    chips = tp // 2
    me = lax.axis_index("tp")
    core, chip = me % 2, me // 2
    x = x.reshape(chips, 2, x.shape[0] // tp, x.shape[1])
    away = lax.dynamic_index_in_dim(x, 1 - core, 1, keepdims=False).astype(jnp.bfloat16)
    keep = lax.dynamic_index_in_dim(x, core, 1, keepdims=False)
    both = keep + swap_core(away).astype(jnp.float32)
    total = lax.dynamic_index_in_dim(both, chip, 0, keepdims=False)
    for r in range(1, chips):
        sent = lax.dynamic_index_in_dim(both, (chip + r) % chips, 0, keepdims=False)
        total = total + shift_chip(sent.astype(jnp.bfloat16), r).astype(jnp.float32)
    return total.astype(jnp.bfloat16)


def diff_kernel(lam_ref, q_ref, k_ref, v_ref, gain_ref, o_ref):
    factor = HEAD ** (-0.5) * math.log2(math.e)
    maps = []
    for m in range(2):
        cols = slice(m * HEAD, (m + 1) * HEAD)
        scores = lax.dot_general(
            q_ref[:, cols], k_ref[:, cols], (((1,), (1,)), ((), ())),
            preferred_element_type=jnp.float32,
        )
        top = jnp.max(scores, axis=-1, keepdims=True)
        expo = jnp.exp2((scores - top) * factor)
        total = jnp.sum(expo, axis=-1, keepdims=True)
        out = jnp.dot(expo.astype(jnp.bfloat16), v_ref[...], preferred_element_type=jnp.float32)
        maps.append(out / total)
    d = maps[0] - lam_ref[pl.program_id(0)] * maps[1]
    d = d * lax.rsqrt(jnp.mean(d * d, axis=-1, keepdims=True) + EPS) * gain_ref[...]
    o_ref[...] = d.astype(jnp.bfloat16)


def diff_attention(q, kv, lam, gain):
    tok, rows, heads = q.shape[0], kv.shape[0], lam.shape[0]
    tile = math.gcd(tok, max(128, 524288 // rows))
    return pl.pallas_call(
        diff_kernel,
        grid=(heads, tok // tile),
        in_specs=[
            pl.BlockSpec(memory_space=pltpu.SMEM),
            pl.BlockSpec((tile, 2 * HEAD), lambda h, i: (i, h)),
            pl.BlockSpec((rows, 2 * HEAD), lambda h, i: (0, h)),
            pl.BlockSpec((rows, VDIM), lambda h, i: (0, heads + h)),
            pl.BlockSpec((1, VDIM), lambda h, i: (0, 0)),
        ],
        out_specs=pl.BlockSpec((tile, VDIM), lambda h, i: (i, h)),
        out_shape=jax.ShapeDtypeStruct((tok, heads * VDIM), jnp.bfloat16),
        cost_estimate=pl.CostEstimate(
            flops=heads * tok * rows * 2 * 2 * (HEAD + VDIM),
            bytes_accessed=2 * (q.size * 2 + kv.size),
            transcendentals=heads * 2 * tok * rows,
        ),
    )(lam, q, kv, kv, gain.reshape(1, VDIM))


def general_body(
    tokens,
    norm_gain,
    query_diff,
    key_diff,
    value_diff,
    lam,
    output_norm_gain,
    query_win,
    keyval_win,
    sink,
    proj_diff,
    proj_win,
):
    bf16, f32 = jnp.bfloat16, jnp.float32
    normed = root_mean_square_rows(tokens.astype(f32), norm_gain).astype(bf16)
    heads_win = sink.shape[0]
    group = WIN_HEADS // KV_HEADS
    n = lax.axis_size("sp")
    me = lax.axis_index("sp")
    parts = lax.axis_size("grp")
    part = lax.axis_index("grp")
    local, width = normed.shape
    depth = width // n
    tok = local * lax.axis_size("tp")

    slabs = normed.reshape(local, n, depth)
    across = jnp.zeros((n, local, depth), bf16)
    own = lax.dynamic_index_in_dim(slabs, me, 1, keepdims=True)
    across = lax.dynamic_update_slice_in_dim(across, jnp.swapaxes(own, 0, 1), me, 0)
    for r in range(1, n):
        sent = lax.dynamic_index_in_dim(slabs, (me + r) % n, 1, keepdims=False)
        got = shifted(sent, "sp", r)
        across = lax.dynamic_update_slice_in_dim(across, got[None], (me - r) % n, 0)

    kv_index = lax.axis_index("tp") * heads_win // group
    kv_local = lax.dynamic_index_in_dim(keyval_win, kv_index, 0, keepdims=False)
    stacked = jnp.concatenate([query_diff, query_win, kv_local], axis=1)
    share = stacked.shape[1] // parts
    half = lax.dynamic_slice_in_dim(stacked, part * share, share, axis=1)
    across, half = lax.optimization_barrier((across, half))

    pieces = [shifted(half, "sp", r) for r in range(1, n)]
    all_rows = gather_tp(across, 1).reshape(n * tok, depth)
    rows_all = gather_tp(normed, 0).reshape(tok, width)
    kv_part = jnp.concatenate(
        [
            jnp.dot(all_rows, key_diff, preferred_element_type=f32).astype(bf16),
            jnp.dot(all_rows, value_diff, preferred_element_type=f32).astype(bf16),
        ],
        axis=1,
    )
    kv = lax.psum_scatter(kv_part, "sp", scatter_dimension=0, tiled=True)
    kv = lax.all_gather(kv, "sp", axis=0, tiled=True)

    own_rows = lax.dynamic_slice_in_dim(rows_all, me * depth, depth, axis=1)
    own_sum = jnp.dot(own_rows, stacked, preferred_element_type=f32)
    sums = [jnp.zeros((tok, share), f32) for _ in range(parts)]
    for r in range(1, n):
        piece = pieces[r - 1]
        rows = lax.dynamic_slice_in_dim(rows_all, (me - r) % n * depth, depth, axis=1)
        for j in range(parts):
            block = piece if j == 0 else shifted(piece, "grp", j)
            sums[j] = sums[j] + jnp.dot(rows, block, preferred_element_type=f32)
    ordered = jnp.stack(sums)
    ordered = jnp.concatenate(
        [
            lax.dynamic_index_in_dim(ordered, (part - b) % parts, 0, keepdims=False)
            for b in range(parts)
        ],
        axis=1,
    )
    projected = (own_sum + ordered).astype(bf16)
    first = query_diff.shape[1]
    second = first + query_win.shape[1]
    q_diff, q_win, kv_win = projected[:, :first], projected[:, first:second], projected[:, second:]
    scale = HEAD ** (-0.5)
    padded = padded_2(kv_win, (("sp", 0),), WINDOW)
    nblocks = tok // WINDOW
    blocks = padded.reshape(nblocks + 2, WINDOW, 2 * HEAD)
    band = jnp.concatenate([blocks[:-2], blocks[1:-1], blocks[2:]], axis=1)
    q_blocks = q_win.reshape(nblocks, WINDOW, heads_win, HEAD)
    scores = (
        jnp.einsum("nqhd,nkd->nhqk", q_blocks, band[..., :HEAD], preferred_element_type=jnp.float32)
        * scale
    )
    q_index = jnp.arange(WINDOW)
    k_index = jnp.arange(3 * WINDOW)
    relative = k_index[None, :] - WINDOW - q_index[:, None]
    first_key = lax.axis_index("sp") * tok - WINDOW
    key_pos = first_key + jnp.arange(nblocks)[:, None] * WINDOW + k_index[None, :]
    inside = (key_pos >= 0) & (key_pos < tok * lax.axis_size("sp"))
    valid = (jnp.abs(relative) <= WINDOW)[None] & inside[:, None, :]
    scores = jnp.where(valid[:, None], scores, -jnp.inf)
    sink_logit = sink[None, :, None, None]
    top_win = jnp.maximum(jnp.max(scores, axis=-1, keepdims=True), sink_logit)
    expo = jnp.exp(scores - top_win)
    weights = expo / (jnp.sum(expo, axis=-1, keepdims=True) + jnp.exp(sink_logit - top_win))
    y_win = jnp.einsum(
        "nhqk,nkd->nqhd",
        weights.astype(jnp.bfloat16),
        band[..., HEAD:],
        preferred_element_type=jnp.float32,
    ).astype(jnp.bfloat16)
    y_win = y_win.reshape(tok, heads_win * HEAD)
    summed = jnp.dot(y_win, proj_win, preferred_element_type=jnp.float32)
    differential_output = diff_attention(q_diff, kv, lam, output_norm_gain)
    summed = summed + jnp.dot(differential_output, proj_diff, preferred_element_type=jnp.float32)
    return scatter_tp(summed)


MESH = pl.DeviceIdType.MESH
CHUNKS = 4
LANES = 128
MATS = 5


def remote(src, dst, send, recv, device):
    return pltpu.make_async_remote_copy(
        src_ref=src, dst_ref=dst, send_sem=send, recv_sem=recv, device_id=device, device_id_type=MESH
    )


def place():
    g, z, t = lax.axis_index("grp"), lax.axis_index("sp"), lax.axis_index("tp")
    x, c = t // 2, t % 2
    return g, z, t, x, c, 2 * (1 - x) + c, 2 * x + 1 - c


def greet(devices):
    barrier = pltpu.get_barrier_semaphore()
    for device in devices:
        pl.semaphore_signal(barrier, inc=1, device_id=device, device_id_type=MESH)
    pl.semaphore_wait(barrier, len(devices))


def arrivals(n, here):
    times = []
    for k in range(1, n):
        for h in range(CHUNKS):
            at = k - 1 + (h + 1) / CHUNKS
            if here - k >= 0:
                times.append((at, "z", here - k, h, 0, k))
            if here + k < n:
                times.append((at + 0.01, "z", here + k, h, 1, k))
    times.sort()
    clock = 0.0
    beside = []
    for at, zz, h in [(0.0, here, h) for h in range(CHUNKS)] + [(e[0], e[2], e[3]) for e in times]:
        clock = max(clock, at) + 1 / CHUNKS
        beside.append((clock + 0.05, "x", zz, h, 0, 0))
    return times + beside


def order(n, here):
    def start(zz):
        return (zz + 1 if zz < here else n - zz, abs(zz - here))

    return sorted((zz for zz in range(n) if zz != here), key=start)


def project_kernel(
    n, held, tok_ref, gain_ref, qd, qw, kd, vd, kvw, pd, pw, scal_ref,
    res_ref, opd, opw, oscal_ref,
    rows_ref, w_ref, sum_ref, zs, zr, xs, xr, cs, cr, ws, wr, ys, yr, own_sem, rs, rr, ps, pr, scal_s, scal_r,
):
    g, z, t, x, c, t_x, t_c = place()
    local, _ = tok_ref.shape
    part = local // CHUNKS
    depth = qd.shape[0]
    half = depth // 2
    group = WIN_HEADS // KV_HEADS
    mats = (qd, qw, kd, vd, kvw)
    core = (g, z, t_c)
    f32, bf16 = jnp.float32, jnp.bfloat16

    def block(zz, h, tt):
        return rows_ref.at[zz, h, pl.ds(pl.multiple_of(tt * part, part), part)]

    for h in range(CHUNKS):
        v = tok_ref[h * part:(h + 1) * part, :].astype(f32)
        v = v * lax.rsqrt(jnp.mean(v * v, axis=-1, keepdims=True) + EPS) * gain_ref[...]
        rows_ref[z, h, pl.ds(pl.multiple_of(t * part, part), part), :] = v.astype(bf16)
    oscal_ref[c] = scal_ref[...]

    greet(
        [(g, lax.rem(z + i // 2, n), 2 * x + (c + i % 2) % 2) for i in range(1, 2 * n)]
        + [(g, z, t_x), (1 - g, z, t)]
    )

    def w_half(zz, yy, m):
        at = pl.ds(pl.multiple_of(zz * depth + yy * half, half), half)
        return w_ref.at[at, m * LANES:(m + 1) * LANES]

    def source(dz, i, cc, m, at):
        if m == MATS - 1:
            return kvw.at[(2 * (x * n + dz)) // group, at, cc * LANES:(cc + 1) * LANES]
        return mats[m].at[at, (2 * i + cc) * LANES:(2 * i + cc + 1) * LANES]

    def w_copy(here, dz, cc, m):
        at = pl.ds(pl.multiple_of(g * half, half), half)
        return remote(
            source(dz, dz % held, cc, m, at), w_half(here, g, m),
            ws.at[dz % held, cc, m], wr.at[here, m], (g, dz, 2 * x + cc),
        )

    def w_each(here, way, act):
        for cs_ in range(2):
            @pl.when(c == cs_)
            def _():
                for m in range(MATS):
                    for dz in range(cs_ * held, (cs_ + 1) * held):
                        if (dz > here) if way == 0 else (dz < here):
                            for cc in range(2):
                                act(w_copy(here, dz, cc, m))

    def own_copy(here, cc, m):
        at = pl.ds(0, depth)
        target = w_ref.at[here * depth:(here + 1) * depth, m * LANES:(m + 1) * LANES]
        return source(here, here % held, cc, m, at), target

    def own_each(here, near, away):
        for cc in range(2):
            for m in range(MATS):
                a, b = own_copy(here, cc, m)

                if near is not None:
                    @pl.when((c == here // held) & (c == cc))
                    def _():
                        near(pltpu.make_async_copy(a, b, own_sem.at[m]))

                @pl.when((c == here // held) & (c != cc))
                def _():
                    away(remote(a, b, ws.at[here % held, cc, m], own_sem.at[m], core))

    def z_copy(zz, h, way, here):
        k = abs(zz - here)
        to = here + 1 if way == 0 else here - 1
        return remote(block(zz, h, t), block(zz, h, t), zs.at[way, k, h], zr.at[way, k + 1, h], (g, to, t))

    def x_copy(zz, h):
        return remote(block(zz, h, t), block(zz, h, t), xs.at[zz, h], xr.at[zz, h], (g, z, t_x))

    def c_copy(zz, xx, h):
        tt = 2 * xx + c
        return remote(block(zz, h, tt), block(zz, h, tt), cs.at[zz, xx, h], cr.at[zz, xx, h], core)

    def y_copy(zz, m):
        return remote(w_half(zz, g, m), w_half(zz, g, m), ys.at[zz, m], yr.at[zz, m], (1 - g, z, t))

    def forward(zz, m):
        remote(w_half(zz, g, m), w_half(zz, g, m), ys.at[zz, m], wr.at[zz, m], core).wait_recv()
        y_copy(zz, m).start()

    def crossed(zz):
        for m in range(MATS):
            remote(w_half(zz, 1 - g, m), w_half(zz, 1 - g, m), ys.at[zz, m], yr.at[zz, m], core).wait_recv()

    scal_copy = remote(scal_ref, oscal_ref.at[c], scal_s, scal_r, core)

    def gather(here):
        for h in range(CHUNKS):
            if here < n - 1:
                z_copy(here, h, 0, here).start()
            if here > 0:
                z_copy(here, h, 1, here).start()
            x_copy(here, h).start()
            c_copy(here, x, h).start()
        scal_copy.start()
        own_each(here, lambda copy: copy.start(), lambda copy: copy.start())
        if here == 0:
            w_each(here, 0, lambda copy: copy.start())
        if here == n - 1:
            w_each(here, 1, lambda copy: copy.start())
        first = order(n, here)[0]
        begin = first + 1 if first < here else n - first
        events = arrivals(n, here)
        events += [(begin + 0.5 * (m + 1), "w", first, m, 0, 0) for m in range(MATS)]
        for at, kind, zz, h, way, k in sorted(events):
            if kind == "z":
                remote(block(zz, h, t), block(zz, h, t), zs.at[way, k, h], zr.at[way, k, h], core).wait_recv()
                if (here < n - 1) if way == 0 else (here > 0):
                    z_copy(zz, h, way, here).start()
                x_copy(zz, h).start()
                c_copy(zz, x, h).start()
                if h == CHUNKS - 1 and zz == (0 if way == 0 else n - 1):
                    w_each(here, way, lambda copy: copy.start())
            elif kind == "x":
                x_copy(zz, h).wait_recv()
                c_copy(zz, 1 - x, h).start()
            else:
                forward(zz, h)

    for here in range(n):
        pl.when(z == here)(functools.partial(gather, here))

    proj_copies = [remote(pd, opd, ps.at[0], pr.at[0], core), remote(pw, opw, ps.at[1], pr.at[1], core)]
    for copy in proj_copies:
        copy.start()

    sources = []
    for j in range(n - 1):
        zz = order(n, 0)[j] + 0 * z
        for here in range(1, n):
            zz = jnp.where(z == here, order(n, here)[j], zz)
        sources.append(zz)

    quad = rows_ref.shape[2]

    def partial_sum(zz, at, size):
        k = pl.ds(pl.multiple_of(at, half), size)
        left = rows_ref[zz, :, :, k].reshape(CHUNKS * quad, size)
        return jnp.dot(left, w_ref[k, :], preferred_element_type=f32)

    def opening(zz, carry):
        for xx in range(2):
            for h in range(CHUNKS):
                c_copy(zz, xx, h).wait_recv()
        sum_ref[zz] = partial_sum(zz, z * depth, depth)
        return carry

    def add(at):
        def one(zz, carry):
            sum_ref[zz] += partial_sum(zz, at, half)
            return carry

        lax.fori_loop(0, n, one, 0)

    def r_copies(zz):
        copies = [remote(
            res_ref.at[c, zz, :, :, 2 * LANES:], res_ref.at[c, zz, :, :, 2 * LANES:],
            rs.at[zz, 0], rr.at[zz, 0], core,
        )]
        for xx in range(2):
            at = pl.ds(pl.multiple_of((2 * xx + 1 - c) * part, part), part)
            copies.append(remote(
                res_ref.at[c, zz, :, at, :2 * LANES], res_ref.at[c, zz, :, at, :2 * LANES],
                rs.at[zz, 1 + xx], rr.at[zz, 1 + xx], core,
            ))
        return copies

    for m in range(MATS):
        a, b = own_copy(0, 0, m)
        pltpu.make_async_copy(a, b, own_sem.at[m]).wait()
    late = sources[1:]

    def forwards(lo, hi):
        for m in range(lo, hi):
            for zz in late:
                forward(zz, m)

    forwards(0, 1)
    lax.fori_loop(0, n, opening, 0)
    forwards(1, 2)
    add(sources[0] * depth + g * half)
    crossed(sources[0])
    add(sources[0] * depth + (1 - g) * half)
    forwards(2, MATS)
    for zz in late:
        add(zz * depth + g * half)
    for zz in late[:-1]:
        crossed(zz)
        add(zz * depth + (1 - g) * half)
    crossed(sources[-1])

    def closing(zz, carry):
        total = sum_ref[zz] + partial_sum(zz, sources[-1] * depth + (1 - g) * half, half)

        @pl.when(zz > 0)
        def _():
            for copy in r_copies(zz - 1):
                copy.start()

        res_ref[c, zz] = total.astype(bf16).reshape(CHUNKS, quad, MATS * LANES)
        return carry

    lax.fori_loop(0, n, closing, 0)
    for copy in proj_copies + [scal_copy]:
        copy.wait()
    for copy in r_copies(n - 1):
        copy.start()

    def drain(here):
        for way in range(2):
            if (here < n - 1) if way == 0 else (here > 0):
                w_each(here, way, lambda copy: copy.wait_send())
                for zz in (range(here + 1) if way == 0 else range(here, n)):
                    for h in range(CHUNKS):
                        z_copy(zz, h, way, here).wait_send()
        own_each(here, None, lambda copy: copy.wait_send())

    for here in range(n):
        pl.when(z == here)(functools.partial(drain, here))

    def finished(zz, carry):
        for h in range(CHUNKS):
            x_copy(zz, h).wait_send()
            for xx in range(2):
                c_copy(zz, xx, h).wait_send()

        @pl.when(zz != z)
        def _():
            for m in range(MATS):
                y_copy(zz, m).wait_send()

        for copy in r_copies(zz):
            copy.wait()
        return carry

    lax.fori_loop(0, n, finished, 0)


def project(n, tokens, norm_gain, query_diff, query_win, key_diff, value_diff, keyval_win, proj_diff, proj_win, scal):
    local, width = tokens.shape
    held = n // 2
    dma = pltpu.SemaphoreType.DMA
    whole = pl.BlockSpec(memory_space=pltpu.VMEM)
    far = pl.BlockSpec(memory_space=pl.ANY)
    cols = MATS * LANES
    tok = 4 * local * n
    return pl.pallas_call(
        functools.partial(project_kernel, n, held),
        in_specs=[whole, whole] + [far] * 7 + [whole],
        out_specs=[whole, far, far, whole],
        out_shape=[
            jax.ShapeDtypeStruct((2, n, CHUNKS, 4 * local // CHUNKS, cols), jnp.bfloat16),
            jax.ShapeDtypeStruct(proj_diff.shape, proj_diff.dtype),
            jax.ShapeDtypeStruct(proj_win.shape, proj_win.dtype),
            jax.ShapeDtypeStruct((2,) + scal.shape, scal.dtype),
        ],
        scratch_shapes=[
            pltpu.VMEM((n, CHUNKS, 4 * local // CHUNKS, width), jnp.bfloat16),
            pltpu.VMEM((width, cols), jnp.bfloat16),
            pltpu.VMEM((n, 4 * local, cols), jnp.float32),
            dma((2, n, CHUNKS)), dma((2, n + 1, CHUNKS)),
            dma((n, CHUNKS)), dma((n, CHUNKS)),
            dma((n, 2, CHUNKS)), dma((n, 2, CHUNKS)),
            dma((held, 2, MATS)), dma((n, MATS)),
            dma((n, MATS)), dma((n, MATS)), dma((MATS,)),
            dma((n, 3)), dma((n, 3)),
            dma((2,)), dma((2,)), dma, dma,
        ],
        compiler_params=pltpu.CompilerParams(
            collective_id=0, has_side_effects=True, vmem_limit_bytes=52 << 20
        ),
        cost_estimate=pl.CostEstimate(
            flops=2 * tok * width * cols, bytes_accessed=2 * width * (tok + cols), transcendentals=0
        ),
    )(tokens, norm_gain.reshape(1, width), query_diff, query_win, key_diff, value_diff, keyval_win, proj_diff, proj_win, scal)


def attend_kernel(n, scal_ref, res_ref, gain_ref, y_ref, v_ref):
    z, t = lax.axis_index("sp"), lax.axis_index("tp")
    c = t % 2
    zz = pl.program_id(0)
    chunks, quad, _ = res_ref.shape[2:]
    part = quad // 4
    local = part * chunks
    rows = n * chunks * quad
    factor = HEAD ** (-0.5) * math.log2(math.e)
    f32, bf16 = jnp.float32, jnp.bfloat16

    @pl.when(zz == 0)
    def _():
        for i in range(2):
            v_ref[:, i * LANES:(i + 1) * LANES] = res_ref[i, :, :, :, 3 * LANES:4 * LANES].reshape(rows, LANES)

    def own(i, xx, m):
        at = pl.ds(pl.multiple_of((2 * xx + c) * part, part), part)
        return res_ref[i, zz, :, at, m * LANES:(m + 1) * LANES].reshape(local, LANES)

    maps = []
    for m in range(2):
        q = jnp.concatenate([own(m, xx, 0) for xx in range(2)], axis=0)
        keys = res_ref[m, :, :, :, 2 * LANES:3 * LANES].reshape(rows, LANES)
        scores = lax.dot_general(q, keys, (((1,), (1,)), ((), ())), preferred_element_type=f32)
        top = jnp.max(scores, axis=-1, keepdims=True)
        expo = jnp.exp2((scores - top) * factor)
        total = jnp.sum(expo, axis=-1, keepdims=True)
        out = jnp.dot(expo.astype(bf16), v_ref[...], preferred_element_type=f32)
        maps.append(out / total)
    lam = scal_ref[z // (n // 2), 0, z % (n // 2)]
    d = maps[0] - lam * maps[1]
    d = d * lax.rsqrt(jnp.mean(d * d, axis=-1, keepdims=True) + EPS) * gain_ref[...]
    y_ref[0, :, :, :VDIM] = d.astype(bf16).reshape(2, local, VDIM)

    held = n // 2
    r_index = lax.broadcasted_iota(jnp.int32, (2 * local, 3 * local), 0) % local
    k_index = lax.broadcasted_iota(jnp.int32, (2 * local, 3 * local), 1)
    near = jnp.abs(k_index - local - r_index) <= WINDOW
    first = lax.broadcasted_iota(jnp.int32, (2 * local, 1), 0) < local
    sinks = [scal_ref[z // held, 1, 2 * (z % held) + i] for i in range(2)]
    sink = jnp.where(first, sinks[0], sinks[1])
    for xx in range(2):
        b = 4 * zz + 2 * xx + c

        def banded(i):
            pieces = []
            for s in (-1, 0, 1):
                o = jnp.clip(b + s, 0, 4 * n - 1)
                at = pl.ds(pl.multiple_of(o % 4 * part, part), part)
                pieces.append(res_ref[i, o // 4, :, at, 4 * LANES:5 * LANES].reshape(local, LANES))
            return jnp.concatenate(pieces, axis=0)

        q = jnp.concatenate([own(i, xx, 1) for i in range(2)], axis=0)
        scores = lax.dot_general(
            q, banded(0), (((1,), (1,)), ((), ())), preferred_element_type=f32
        ) * HEAD ** (-0.5)
        spot = (b - 1) * local + k_index
        valid = near & (spot >= 0) & (spot < rows)
        scores = jnp.where(valid, scores, -jnp.inf)
        top = jnp.maximum(jnp.max(scores, axis=-1, keepdims=True), sink)
        expo = jnp.exp(scores - top)
        weights = expo / (jnp.sum(expo, axis=-1, keepdims=True) + jnp.exp(sink - top))
        out = jnp.dot(weights.astype(bf16), banded(1), preferred_element_type=f32).astype(bf16)
        for i in range(2):
            y_ref[0, xx, :, VDIM + i * LANES:VDIM + (i + 1) * LANES] = out[i * local:(i + 1) * local]


def attend(n, scal, res, gain):
    chunks, quad, _ = res.shape[2:]
    local = quad * chunks // 4
    rows = n * chunks * quad
    feats = VDIM + 2 * HEAD
    return pl.pallas_call(
        functools.partial(attend_kernel, n),
        grid=(n,),
        in_specs=[
            pl.BlockSpec(memory_space=pltpu.SMEM),
            pl.BlockSpec(memory_space=pltpu.VMEM),
            pl.BlockSpec(memory_space=pltpu.VMEM),
        ],
        out_specs=pl.BlockSpec((1, 2, local, feats), lambda i: (i, 0, 0, 0)),
        out_shape=jax.ShapeDtypeStruct((n, 2, local, feats), jnp.bfloat16),
        scratch_shapes=[pltpu.VMEM((rows, VDIM), jnp.bfloat16)],
        cost_estimate=pl.CostEstimate(
            flops=rows * rows * 2 * (HEAD + VDIM), bytes_accessed=2 * res.size, transcendentals=rows * rows
        ),
    )(scal, res, gain.reshape(1, VDIM))


def finish_kernel(
    n, y_ref, pd, pw, opd, opw, out_ref,
    got_ref, p_ref, mine_ref, away_ref, theirs_ref, ys, yr, load, ds, dr,
):
    g, z, t, x, c, t_x, _ = place()
    held = n // 2
    local, width = out_ref.shape
    steps = mine_ref.shape[0]
    wide = width // steps
    f32, bf16 = jnp.float32, jnp.bfloat16

    loads = []
    for i in range(held):
        for far, at, a, b in ((0, c, pd, pw), (1, 1 - c, opd, opw)):
            for j, ref in enumerate((a, b)):
                loads.append(pltpu.make_async_copy(
                    ref.at[i * VDIM:(i + 1) * VDIM], p_ref.at[at * held + i, j * VDIM:(j + 1) * VDIM],
                    load.at[i, far, j],
                ))
    for copy in loads:
        copy.start()

    greet([(g, lax.rem(z + i, n), t) for i in range(1, n)] + [(g, z, t_x)])

    def y_copy(zz, xx):
        return remote(y_ref.at[zz, xx], got_ref.at[z, xx], ys.at[zz, xx], yr.at[z, xx], (g, zz, t))

    def y_wait(zz, xx):
        return remote(got_ref.at[zz, xx], got_ref.at[zz, xx], ys.at[zz, xx], yr.at[zz, xx], (g, z, t_x))

    def others(act):
        for d in range(n - 1, 0, -1):
            pl.when(z - d >= 0)(functools.partial(act, z - d))
            pl.when(z + d < n)(functools.partial(act, z + d))

    for xx in (1 - x, x):
        others(lambda zz: y_copy(zz, xx).start())
    got_ref[z] = y_ref[z]
    for copy in loads:
        copy.wait()

    def product(j, xx):
        total = jnp.zeros((local, wide), f32)
        at = pl.ds(pl.multiple_of(j * wide, wide), wide)
        for zz in range(n):
            total = total + jnp.dot(got_ref[zz, xx], p_ref[zz, :, at], preferred_element_type=f32)
        return total

    def d_copy(j):
        return remote(away_ref.at[j], theirs_ref.at[j], ds.at[j], dr.at[j], (g, z, t_x))

    others(lambda zz: y_wait(zz, 1 - x).wait_recv())

    def send(j, carry):
        value = product(j, 1 - x).astype(bf16)

        @pl.when(j > 0)
        def _():
            d_copy(j - 1).start()

        away_ref[j] = value
        return carry

    lax.fori_loop(0, steps, send, 0)
    others(lambda zz: y_wait(zz, x).wait_recv())
    d_copy(steps - 1).start()

    def keep(j, carry):
        mine_ref[j] = product(j, x)
        return carry

    lax.fori_loop(0, steps, keep, 0)
    for j in range(steps):
        d_copy(j).wait_recv()
        out_ref[:, j * wide:(j + 1) * wide] = (mine_ref[j] + theirs_ref[j].astype(f32)).astype(bf16)
    for j in range(steps):
        d_copy(j).wait_send()
    for xx in (1 - x, x):
        others(lambda zz: y_copy(zz, xx).wait_send())


def finish(n, y, proj_diff, proj_win, other_diff, other_win):
    local, feats = y.shape[2:]
    width = proj_diff.shape[1]
    steps = 8
    dma = pltpu.SemaphoreType.DMA
    whole = pl.BlockSpec(memory_space=pltpu.VMEM)
    far = pl.BlockSpec(memory_space=pl.ANY)
    return pl.pallas_call(
        functools.partial(finish_kernel, n),
        in_specs=[whole] + [far] * 4,
        out_specs=whole,
        out_shape=jax.ShapeDtypeStruct((local, width), jnp.bfloat16),
        scratch_shapes=[
            pltpu.VMEM(y.shape, jnp.bfloat16),
            pltpu.VMEM((n, feats, width), jnp.bfloat16),
            pltpu.VMEM((steps, local, width // steps), jnp.float32),
            pltpu.VMEM((steps, local, width // steps), jnp.bfloat16),
            pltpu.VMEM((steps, local, width // steps), jnp.bfloat16),
            dma((n, 2)), dma((n, 2)), dma((n // 2, 2, 2)), dma((steps,)), dma((steps,)),
        ],
        compiler_params=pltpu.CompilerParams(
            collective_id=1, has_side_effects=True, vmem_limit_bytes=52 << 20
        ),
        cost_estimate=pl.CostEstimate(
            flops=2 * 2 * local * n * feats * width, bytes_accessed=2 * n * feats * width, transcendentals=0
        ),
    )(y, proj_diff, proj_win, other_diff, other_win)


def split_body(
    tokens, norm_gain, query_diff, key_diff, value_diff, lam, output_norm_gain,
    query_win, keyval_win, sink, proj_diff, proj_win,
):
    n = lax.axis_size("sp")
    scal = jnp.stack([jnp.pad(lam, (0, LANES - lam.shape[0])), jnp.pad(sink, (0, LANES - sink.shape[0]))])
    scal = jnp.pad(scal, ((0, 6), (0, 0)))
    res, other_diff, other_win, both = project(
        n, tokens, norm_gain, query_diff, query_win, key_diff, value_diff, keyval_win, proj_diff, proj_win, scal
    )
    y = attend(n, both, res, output_norm_gain)
    return finish(n, y, proj_diff, proj_win, other_diff, other_win)


def splits(mesh, tokens, query_diff, query_win, lam, sink):
    parts, n, tp = (mesh.shape[a] for a in ("grp", "sp", "tp"))
    return (
        parts == 2 and tp == 4 and n % 2 == 0
        and lam.shape[0] == 2 * n and sink.shape[0] == 2 * lam.shape[0]
        and tokens.shape[0] == parts * n * tp * WINDOW
        and query_diff.shape[1] == lam.shape[0] * 2 * HEAD and VDIM == 2 * HEAD
        and query_win.shape[1] == sink.shape[0] * HEAD and HEAD == LANES
    )


def solution(mesh):
    placed = (
        P(("grp", "sp", "tp"), None),
        P(),
        P("sp", "tp"),
        P("sp", "tp"),
        P("sp", "tp"),
        P("tp"),
        P(),
        P("sp", "tp"),
        P(None, "sp", None),
        P("tp"),
        P("tp", None),
        P("tp", None),
    )

    def build(body):
        return jax.shard_map(
            body, mesh=mesh, in_specs=placed, out_specs=P(("grp", "sp", "tp"), None), check_vma=False
        )

    general = build(general_body)

    def step(*args):
        tokens, query_diff, lam, query_win, sink = (args[i] for i in (0, 2, 5, 7, 9))
        if splits(mesh, tokens, query_diff, query_win, lam, sink):
            return build(split_body)(*args)
        return general(*args)

    return step
```

```python
import functools
import math

import jax
import jax.numpy as jnp
from jax import lax
from jax.experimental import pallas as pl
from jax.experimental.pallas import tpu as pltpu
from jax.sharding import PartitionSpec as P


HEAD = 128
WIN_HEADS = 16
KV_HEADS = 4
WINDOW = 128
VDIM = 256


EPS = 1e-06


def padded_2(x, sides, width):
    for axis, dim in sides:
        devices, length = (lax.axis_size(axis), x.shape[dim])
        up = [(i, (i + 1) % devices) for i in range(devices - 1)]
        down = [(j, i) for i, j in up]
        last = lax.slice_in_dim(x, length - width, length, axis=dim)
        first = lax.slice_in_dim(x, 0, width, axis=dim)
        before = lax.ppermute(last, axis, up)
        after = lax.ppermute(first, axis, down)
        x = jnp.concatenate([before, x, after], axis=dim)
    return x


def root_mean_square_rows(values, gain):
    return values * lax.rsqrt(jnp.mean(values * values, axis=-1, keepdims=True) + EPS) * gain


def shifted(x, axis, by):
    n = lax.axis_size(axis)
    return lax.ppermute(x, axis, [(i, (i + by) % n) for i in range(n)])


def shift_chip(x, by):
    n = lax.axis_size("tp")
    return lax.ppermute(x, "tp", [(i, (i + 2 * by) % n) for i in range(n)])


def swap_core(x):
    n = lax.axis_size("tp")
    return lax.ppermute(x, "tp", [(i, i ^ 1) for i in range(n)])


def gather_tp(x, axis):
    tp = lax.axis_size("tp")
    chips = tp // 2
    me = lax.axis_index("tp")
    mine = [x] + [shift_chip(x, r) for r in range(1, chips)]
    theirs = [swap_core(piece) for piece in mine]
    out = jnp.zeros(x.shape[:axis] + (tp,) + x.shape[axis:], x.dtype)
    for r in range(chips):
        at = (me - 2 * r) % tp
        out = lax.dynamic_update_slice_in_dim(out, jnp.expand_dims(mine[r], axis), at, axis)
        out = lax.dynamic_update_slice_in_dim(out, jnp.expand_dims(theirs[r], axis), at ^ 1, axis)
    return out


def scatter_tp(x):
    tp = lax.axis_size("tp")
    chips = tp // 2
    me = lax.axis_index("tp")
    core, chip = me % 2, me // 2
    x = x.reshape(chips, 2, x.shape[0] // tp, x.shape[1])
    away = lax.dynamic_index_in_dim(x, 1 - core, 1, keepdims=False).astype(jnp.bfloat16)
    keep = lax.dynamic_index_in_dim(x, core, 1, keepdims=False)
    both = keep + swap_core(away).astype(jnp.float32)
    total = lax.dynamic_index_in_dim(both, chip, 0, keepdims=False)
    for r in range(1, chips):
        sent = lax.dynamic_index_in_dim(both, (chip + r) % chips, 0, keepdims=False)
        total = total + shift_chip(sent.astype(jnp.bfloat16), r).astype(jnp.float32)
    return total.astype(jnp.bfloat16)


def diff_kernel(lam_ref, q_ref, k_ref, v_ref, gain_ref, o_ref):
    factor = HEAD ** (-0.5) * math.log2(math.e)
    maps = []
    for m in range(2):
        cols = slice(m * HEAD, (m + 1) * HEAD)
        scores = lax.dot_general(
            q_ref[:, cols], k_ref[:, cols], (((1,), (1,)), ((), ())),
            preferred_element_type=jnp.float32,
        )
        top = jnp.max(scores, axis=-1, keepdims=True)
        expo = jnp.exp2((scores - top) * factor)
        total = jnp.sum(expo, axis=-1, keepdims=True)
        out = jnp.dot(expo.astype(jnp.bfloat16), v_ref[...], preferred_element_type=jnp.float32)
        maps.append(out / total)
    d = maps[0] - lam_ref[pl.program_id(0)] * maps[1]
    d = d * lax.rsqrt(jnp.mean(d * d, axis=-1, keepdims=True) + EPS) * gain_ref[...]
    o_ref[...] = d.astype(jnp.bfloat16)


def diff_attention(q, kv, lam, gain):
    tok, rows, heads = q.shape[0], kv.shape[0], lam.shape[0]
    tile = math.gcd(tok, max(128, 524288 // rows))
    return pl.pallas_call(
        diff_kernel,
        grid=(heads, tok // tile),
        in_specs=[
            pl.BlockSpec(memory_space=pltpu.SMEM),
            pl.BlockSpec((tile, 2 * HEAD), lambda h, i: (i, h)),
            pl.BlockSpec((rows, 2 * HEAD), lambda h, i: (0, h)),
            pl.BlockSpec((rows, VDIM), lambda h, i: (0, heads + h)),
            pl.BlockSpec((1, VDIM), lambda h, i: (0, 0)),
        ],
        out_specs=pl.BlockSpec((tile, VDIM), lambda h, i: (i, h)),
        out_shape=jax.ShapeDtypeStruct((tok, heads * VDIM), jnp.bfloat16),
        cost_estimate=pl.CostEstimate(
            flops=heads * tok * rows * 2 * 2 * (HEAD + VDIM),
            bytes_accessed=2 * (q.size * 2 + kv.size),
            transcendentals=heads * 2 * tok * rows,
        ),
    )(lam, q, kv, kv, gain.reshape(1, VDIM))


def general_body(
    tokens,
    norm_gain,
    query_diff,
    key_diff,
    value_diff,
    lam,
    output_norm_gain,
    query_win,
    keyval_win,
    sink,
    proj_diff,
    proj_win,
):
    bf16, f32 = jnp.bfloat16, jnp.float32
    normed = root_mean_square_rows(tokens.astype(f32), norm_gain).astype(bf16)
    heads_win = sink.shape[0]
    group = WIN_HEADS // KV_HEADS
    n = lax.axis_size("sp")
    me = lax.axis_index("sp")
    parts = lax.axis_size("grp")
    part = lax.axis_index("grp")
    local, width = normed.shape
    depth = width // n
    tok = local * lax.axis_size("tp")

    slabs = normed.reshape(local, n, depth)
    across = jnp.zeros((n, local, depth), bf16)
    own = lax.dynamic_index_in_dim(slabs, me, 1, keepdims=True)
    across = lax.dynamic_update_slice_in_dim(across, jnp.swapaxes(own, 0, 1), me, 0)
    for r in range(1, n):
        sent = lax.dynamic_index_in_dim(slabs, (me + r) % n, 1, keepdims=False)
        got = shifted(sent, "sp", r)
        across = lax.dynamic_update_slice_in_dim(across, got[None], (me - r) % n, 0)

    kv_index = lax.axis_index("tp") * heads_win // group
    kv_local = lax.dynamic_index_in_dim(keyval_win, kv_index, 0, keepdims=False)
    stacked = jnp.concatenate([query_diff, query_win, kv_local], axis=1)
    share = stacked.shape[1] // parts
    half = lax.dynamic_slice_in_dim(stacked, part * share, share, axis=1)
    across, half = lax.optimization_barrier((across, half))

    pieces = [shifted(half, "sp", r) for r in range(1, n)]
    all_rows = gather_tp(across, 1).reshape(n * tok, depth)
    rows_all = gather_tp(normed, 0).reshape(tok, width)
    kv_part = jnp.concatenate(
        [
            jnp.dot(all_rows, key_diff, preferred_element_type=f32).astype(bf16),
            jnp.dot(all_rows, value_diff, preferred_element_type=f32).astype(bf16),
        ],
        axis=1,
    )
    kv = lax.psum_scatter(kv_part, "sp", scatter_dimension=0, tiled=True)
    kv = lax.all_gather(kv, "sp", axis=0, tiled=True)

    own_rows = lax.dynamic_slice_in_dim(rows_all, me * depth, depth, axis=1)
    own_sum = jnp.dot(own_rows, stacked, preferred_element_type=f32)
    sums = [jnp.zeros((tok, share), f32) for _ in range(parts)]
    for r in range(1, n):
        piece = pieces[r - 1]
        rows = lax.dynamic_slice_in_dim(rows_all, (me - r) % n * depth, depth, axis=1)
        for j in range(parts):
            block = piece if j == 0 else shifted(piece, "grp", j)
            sums[j] = sums[j] + jnp.dot(rows, block, preferred_element_type=f32)
    ordered = jnp.stack(sums)
    ordered = jnp.concatenate(
        [
            lax.dynamic_index_in_dim(ordered, (part - b) % parts, 0, keepdims=False)
            for b in range(parts)
        ],
        axis=1,
    )
    projected = (own_sum + ordered).astype(bf16)
    first = query_diff.shape[1]
    second = first + query_win.shape[1]
    q_diff, q_win, kv_win = projected[:, :first], projected[:, first:second], projected[:, second:]
    scale = HEAD ** (-0.5)
    padded = padded_2(kv_win, (("sp", 0),), WINDOW)
    nblocks = tok // WINDOW
    blocks = padded.reshape(nblocks + 2, WINDOW, 2 * HEAD)
    band = jnp.concatenate([blocks[:-2], blocks[1:-1], blocks[2:]], axis=1)
    q_blocks = q_win.reshape(nblocks, WINDOW, heads_win, HEAD)
    scores = (
        jnp.einsum("nqhd,nkd->nhqk", q_blocks, band[..., :HEAD], preferred_element_type=jnp.float32)
        * scale
    )
    q_index = jnp.arange(WINDOW)
    k_index = jnp.arange(3 * WINDOW)
    relative = k_index[None, :] - WINDOW - q_index[:, None]
    first_key = lax.axis_index("sp") * tok - WINDOW
    key_pos = first_key + jnp.arange(nblocks)[:, None] * WINDOW + k_index[None, :]
    inside = (key_pos >= 0) & (key_pos < tok * lax.axis_size("sp"))
    valid = (jnp.abs(relative) <= WINDOW)[None] & inside[:, None, :]
    scores = jnp.where(valid[:, None], scores, -jnp.inf)
    sink_logit = sink[None, :, None, None]
    top_win = jnp.maximum(jnp.max(scores, axis=-1, keepdims=True), sink_logit)
    expo = jnp.exp(scores - top_win)
    weights = expo / (jnp.sum(expo, axis=-1, keepdims=True) + jnp.exp(sink_logit - top_win))
    y_win = jnp.einsum(
        "nhqk,nkd->nqhd",
        weights.astype(jnp.bfloat16),
        band[..., HEAD:],
        preferred_element_type=jnp.float32,
    ).astype(jnp.bfloat16)
    y_win = y_win.reshape(tok, heads_win * HEAD)
    summed = jnp.dot(y_win, proj_win, preferred_element_type=jnp.float32)
    differential_output = diff_attention(q_diff, kv, lam, output_norm_gain)
    summed = summed + jnp.dot(differential_output, proj_diff, preferred_element_type=jnp.float32)
    return scatter_tp(summed)


MESH = pl.DeviceIdType.MESH
CHUNKS = 4
LANES = 128
MATS = 5


def remote(src, dst, send, recv, device):
    return pltpu.make_async_remote_copy(
        src_ref=src, dst_ref=dst, send_sem=send, recv_sem=recv, device_id=device, device_id_type=MESH
    )


def place():
    g, z, t = lax.axis_index("grp"), lax.axis_index("sp"), lax.axis_index("tp")
    x, c = t // 2, t % 2
    return g, z, t, x, c, 2 * (1 - x) + c, 2 * x + 1 - c


def greet(devices):
    barrier = pltpu.get_barrier_semaphore()
    for device in devices:
        pl.semaphore_signal(barrier, inc=1, device_id=device, device_id_type=MESH)
    pl.semaphore_wait(barrier, len(devices))


def arrivals(n, here):
    times = []
    for k in range(1, n):
        for h in range(CHUNKS):
            at = k - 1 + (h + 1) / CHUNKS
            if here - k >= 0:
                times.append((at, "z", here - k, h, 0, k))
            if here + k < n:
                times.append((at + 0.01, "z", here + k, h, 1, k))
    times.sort()
    clock = 0.0
    beside = []
    for at, zz, h in [(0.0, here, h) for h in range(CHUNKS)] + [(e[0], e[2], e[3]) for e in times]:
        clock = max(clock, at) + 1 / CHUNKS
        beside.append((clock + 0.05, "x", zz, h, 0, 0))
    return times + beside


def order(n, here):
    def start(zz):
        return (zz + 1 if zz < here else n - zz, abs(zz - here))

    return sorted((zz for zz in range(n) if zz != here), key=start)


def whole_kernel(
    n, held, tok_ref, gain_ref, qd, qw, kd, vd, kvw, pd, pw, scal_ref, out_gain_ref,
    out_ref,
    rows_ref, w_ref, sum_ref, res_ref, oscal_ref, p_ref, v_ref, y_ref, got_ref, mine_ref, away_ref, theirs_ref,
    zs, zr, xs, xr, cs, cr, ws, wr, ys, yr, own_sem, rs, rr, ps, pr, load, scal_s, scal_r, hs, hr, ds, dr,
):
    g, z, t, x, c, t_x, t_c = place()
    local, width = tok_ref.shape
    part = local // CHUNKS
    depth = qd.shape[0]
    half = depth // 2
    group = WIN_HEADS // KV_HEADS
    mats = (qd, qw, kd, vd, kvw)
    core = (g, z, t_c)
    f32, bf16 = jnp.float32, jnp.bfloat16

    def block(zz, h, tt):
        return rows_ref.at[zz, h, pl.ds(pl.multiple_of(tt * part, part), part)]

    for h in range(CHUNKS):
        v = tok_ref[h * part:(h + 1) * part, :].astype(f32)
        v = v * lax.rsqrt(jnp.mean(v * v, axis=-1, keepdims=True) + EPS) * gain_ref[...]
        rows_ref[z, h, pl.ds(pl.multiple_of(t * part, part), part), :] = v.astype(bf16)
    oscal_ref[c] = scal_ref[...]

    greet(
        [(g, lax.rem(z + i // 2, n), 2 * x + (c + i % 2) % 2) for i in range(1, 2 * n)]
        + [(g, z, t_x), (1 - g, z, t)]
    )

    def w_half(zz, yy, m):
        at = pl.ds(pl.multiple_of(zz * depth + yy * half, half), half)
        return w_ref.at[at, m * LANES:(m + 1) * LANES]

    def source(dz, i, cc, m, at):
        if m == MATS - 1:
            return kvw.at[(2 * (x * n + dz)) // group, at, cc * LANES:(cc + 1) * LANES]
        return mats[m].at[at, (2 * i + cc) * LANES:(2 * i + cc + 1) * LANES]

    def w_copy(here, dz, cc, m):
        at = pl.ds(pl.multiple_of(g * half, half), half)
        return remote(
            source(dz, dz % held, cc, m, at), w_half(here, g, m),
            ws.at[dz % held, cc, m], wr.at[here, m], (g, dz, 2 * x + cc),
        )

    def w_each(here, way, act):
        for cs_ in range(2):
            @pl.when(c == cs_)
            def _():
                for m in range(MATS):
                    for dz in range(cs_ * held, (cs_ + 1) * held):
                        if (dz > here) if way == 0 else (dz < here):
                            for cc in range(2):
                                act(w_copy(here, dz, cc, m))

    def own_copy(here, cc, m):
        at = pl.ds(0, depth)
        target = w_ref.at[here * depth:(here + 1) * depth, m * LANES:(m + 1) * LANES]
        return source(here, here % held, cc, m, at), target

    def own_each(here, near, away):
        for cc in range(2):
            for m in range(MATS):
                a, b = own_copy(here, cc, m)

                if near is not None:
                    @pl.when((c == here // held) & (c == cc))
                    def _():
                        near(pltpu.make_async_copy(a, b, own_sem.at[m]))

                @pl.when((c == here // held) & (c != cc))
                def _():
                    away(remote(a, b, ws.at[here % held, cc, m], own_sem.at[m], core))

    def z_copy(zz, h, way, here):
        k = abs(zz - here)
        to = here + 1 if way == 0 else here - 1
        return remote(block(zz, h, t), block(zz, h, t), zs.at[way, k, h], zr.at[way, k + 1, h], (g, to, t))

    def x_copy(zz, h):
        return remote(block(zz, h, t), block(zz, h, t), xs.at[zz, h], xr.at[zz, h], (g, z, t_x))

    def c_copy(zz, xx, h):
        tt = 2 * xx + c
        return remote(block(zz, h, tt), block(zz, h, tt), cs.at[zz, xx, h], cr.at[zz, xx, h], core)

    def y_copy(zz, m):
        return remote(w_half(zz, g, m), w_half(zz, g, m), ys.at[zz, m], yr.at[zz, m], (1 - g, z, t))

    def forward(zz, m):
        remote(w_half(zz, g, m), w_half(zz, g, m), ys.at[zz, m], wr.at[zz, m], core).wait_recv()
        y_copy(zz, m).start()

    def crossed(zz):
        for m in range(MATS):
            remote(w_half(zz, 1 - g, m), w_half(zz, 1 - g, m), ys.at[zz, m], yr.at[zz, m], core).wait_recv()

    scal_copy = remote(scal_ref, oscal_ref.at[c], scal_s, scal_r, core)

    def gather(here):
        for h in range(CHUNKS):
            if here < n - 1:
                z_copy(here, h, 0, here).start()
            if here > 0:
                z_copy(here, h, 1, here).start()
            x_copy(here, h).start()
            c_copy(here, x, h).start()
        scal_copy.start()
        own_each(here, lambda copy: copy.start(), lambda copy: copy.start())
        if here == 0:
            w_each(here, 0, lambda copy: copy.start())
        if here == n - 1:
            w_each(here, 1, lambda copy: copy.start())
        first = order(n, here)[0]
        begin = first + 1 if first < here else n - first
        events = arrivals(n, here)
        events += [(begin + 0.5 * (m + 1), "w", first, m, 0, 0) for m in range(MATS)]
        for at, kind, zz, h, way, k in sorted(events):
            if kind == "z":
                remote(block(zz, h, t), block(zz, h, t), zs.at[way, k, h], zr.at[way, k, h], core).wait_recv()
                if (here < n - 1) if way == 0 else (here > 0):
                    z_copy(zz, h, way, here).start()
                x_copy(zz, h).start()
                c_copy(zz, x, h).start()
                if h == CHUNKS - 1 and zz == (0 if way == 0 else n - 1):
                    w_each(here, way, lambda copy: copy.start())
            elif kind == "x":
                x_copy(zz, h).wait_recv()
                c_copy(zz, 1 - x, h).start()
            else:
                forward(zz, h)

    for here in range(n):
        pl.when(z == here)(functools.partial(gather, here))

    proj_copies, loads = [], []
    for i in range(held):
        for j, ref in enumerate((pd, pw)):
            rows = ref.at[i * VDIM:(i + 1) * VDIM]
            at = p_ref.at[c * held + i, j * VDIM:(j + 1) * VDIM]
            loads.append(pltpu.make_async_copy(rows, at, load.at[i, j]))
            proj_copies.append(remote(rows, at, ps.at[i, j], pr.at[i, j], core))
    for copy in loads + proj_copies:
        copy.start()

    sources = []
    for j in range(n - 1):
        zz = order(n, 0)[j] + 0 * z
        for here in range(1, n):
            zz = jnp.where(z == here, order(n, here)[j], zz)
        sources.append(zz)

    quad = rows_ref.shape[2]

    def partial_sum(zz, at, size):
        k = pl.ds(pl.multiple_of(at, half), size)
        left = rows_ref[zz, :, :, k].reshape(CHUNKS * quad, size)
        return jnp.dot(left, w_ref[k, :], preferred_element_type=f32)

    def opening(zz, carry):
        for xx in range(2):
            for h in range(CHUNKS):
                c_copy(zz, xx, h).wait_recv()
        sum_ref[zz] = partial_sum(zz, z * depth, depth)
        return carry

    def add(at):
        def one(zz, carry):
            sum_ref[zz] += partial_sum(zz, at, half)
            return carry

        lax.fori_loop(0, n, one, 0)

    def r_copies(zz):
        copies = [remote(
            res_ref.at[c, zz, :, :, 2 * LANES:], res_ref.at[c, zz, :, :, 2 * LANES:],
            rs.at[zz, 0], rr.at[zz, 0], core,
        )]
        for xx in range(2):
            at = pl.ds(pl.multiple_of((2 * xx + 1 - c) * part, part), part)
            copies.append(remote(
                res_ref.at[c, zz, :, at, :2 * LANES], res_ref.at[c, zz, :, at, :2 * LANES],
                rs.at[zz, 1 + xx], rr.at[zz, 1 + xx], core,
            ))
        return copies

    for m in range(MATS):
        a, b = own_copy(0, 0, m)
        pltpu.make_async_copy(a, b, own_sem.at[m]).wait()
    late = sources[1:]

    def forwards(lo, hi):
        for m in range(lo, hi):
            for zz in late:
                forward(zz, m)

    forwards(0, 1)
    lax.fori_loop(0, n, opening, 0)
    forwards(1, 2)
    add(sources[0] * depth + g * half)
    crossed(sources[0])
    add(sources[0] * depth + (1 - g) * half)
    forwards(2, MATS)
    for zz in late:
        add(zz * depth + g * half)
    for zz in late[:-1]:
        crossed(zz)
        add(zz * depth + (1 - g) * half)
    crossed(sources[-1])

    def closing(zz, carry):
        total = sum_ref[zz] + partial_sum(zz, sources[-1] * depth + (1 - g) * half, half)

        @pl.when(zz > 0)
        def _():
            for copy in r_copies(zz - 1):
                copy.start()

        res_ref[c, zz] = total.astype(bf16).reshape(CHUNKS, quad, MATS * LANES)
        return carry

    lax.fori_loop(0, n, closing, 0)
    scal_copy.wait()
    for copy in r_copies(n - 1):
        copy.start()

    def exchanged(zz, carry):
        for copy in r_copies(zz):
            copy.wait_recv()
        return carry

    lax.fori_loop(0, n, exchanged, 0)

    rows = n * 4 * local
    factor = HEAD ** (-0.5) * math.log2(math.e)
    for i in range(2):
        v_ref[:, i * LANES:(i + 1) * LANES] = res_ref[i, :, :, :, 3 * LANES:4 * LANES].reshape(rows, LANES)

    level = oscal_ref[z // held]
    level_row = lax.broadcasted_iota(jnp.int32, level.shape, 0)
    level_lane = lax.broadcasted_iota(jnp.int32, level.shape, 1)

    def scalar(row, lane):
        picked = jnp.where((level_row == row) & (level_lane == lane), level, 0.0)
        return jnp.sum(jnp.sum(picked, axis=1, keepdims=True), axis=0, keepdims=True)

    lam = scalar(0, z % held)
    sinks = [scalar(1, 2 * (z % held) + i) for i in range(2)]
    first = lax.broadcasted_iota(jnp.int32, (2 * local, 1), 0) < local
    sink = jnp.where(first, sinks[0], sinks[1])

    distant = []
    for j in range(n):
        zz = 0 * z
        for here in range(n):
            far = sorted(range(n), key=lambda o: -abs(o - here))[j]
            zz = jnp.where(z == here, far, zz)
        distant.append(zz)

    def pick(values, j):
        value = values[0]
        for i in range(1, len(values)):
            value = jnp.where(j == i, values[i], value)
        return value

    def piece(i, zz, tt, m):
        at = pl.ds(pl.multiple_of(tt * part, part), part)
        return res_ref[i, zz, :, at, m * LANES:(m + 1) * LANES].reshape(local, LANES)

    def y_copy_to(zz, xx):
        return remote(y_ref.at[zz, xx], got_ref.at[z, xx], hs.at[zz, xx], hr.at[z, xx], (g, zz, t))

    def y_wait(zz, xx):
        return remote(got_ref.at[zz, xx], got_ref.at[zz, xx], hs.at[zz, xx], hr.at[zz, xx], (g, z, t_x))

    def windowed(zz, tt, xx):
        b = 4 * zz + tt

        def banded(i):
            pieces = []
            for o in (-1, 0, 1):
                o = jnp.clip(b + o, 0, 4 * n - 1)
                pieces.append(piece(i, o // 4, o % 4, 4))
            return jnp.concatenate(pieces, axis=0)

        q = jnp.concatenate([piece(i, zz, tt, 1) for i in range(2)], axis=0)
        scores = lax.dot_general(
            q, banded(0), (((1,), (1,)), ((), ())), preferred_element_type=f32
        ) * HEAD ** (-0.5)
        r_index = lax.broadcasted_iota(jnp.int32, scores.shape, 0) % local
        k_index = lax.broadcasted_iota(jnp.int32, scores.shape, 1)
        spot = (b - 1) * local + k_index
        valid = (jnp.abs(k_index - local - r_index) <= WINDOW) & (spot >= 0) & (spot < rows)
        scores = jnp.where(valid, scores, -jnp.inf)
        top = jnp.maximum(jnp.max(scores, axis=-1, keepdims=True), sink)
        expo = jnp.exp(scores - top)
        weights = expo / (jnp.sum(expo, axis=-1, keepdims=True) + jnp.exp(sink - top))
        out = jnp.dot(weights.astype(bf16), banded(1), preferred_element_type=f32).astype(bf16)
        for i in range(2):
            y_ref[zz, xx, :, VDIM + i * LANES:VDIM + (i + 1) * LANES] = out[i * local:(i + 1) * local]

    def attend(step, carry):
        pairs = n // 2
        xx = jnp.where(step < pairs, 1 - x, x)
        tt = 2 * xx + c
        j = step % pairs
        zzs = [pick(distant[i::2], j) for i in range(2)]
        maps = []
        for m in range(2):
            q = jnp.concatenate([piece(m, zz, tt, 0) for zz in zzs], axis=0)
            keys = res_ref[m, :, :, :, 2 * LANES:3 * LANES].reshape(rows, LANES)
            scores = lax.dot_general(q, keys, (((1,), (1,)), ((), ())), preferred_element_type=f32)
            top = jnp.max(scores, axis=-1, keepdims=True)
            expo = jnp.exp2((scores - top) * factor)
            total = jnp.sum(expo, axis=-1, keepdims=True)
            out = jnp.dot(expo.astype(bf16), v_ref[...], preferred_element_type=f32)
            maps.append(out / total)
        d = maps[0] - lam * maps[1]
        d = d * lax.rsqrt(jnp.mean(d * d, axis=-1, keepdims=True) + EPS) * out_gain_ref[...]
        d = d.astype(bf16)
        for i, zz in enumerate(zzs):
            y_ref[zz, xx, :, :VDIM] = d[i * local:(i + 1) * local]
        for zz in zzs:
            windowed(zz, tt, xx)
        for zz in zzs:
            @pl.when(zz != z)
            def _():
                y_copy_to(zz, xx).start()
        return carry

    lax.fori_loop(0, n, attend, 0)
    got_ref[z] = y_ref[z]
    for copy in loads + proj_copies:
        copy.wait()

    steps = mine_ref.shape[0]
    wide = width // steps

    def others(act):
        for d in range(n - 1, 0, -1):
            pl.when(z - d >= 0)(functools.partial(act, z - d))
            pl.when(z + d < n)(functools.partial(act, z + d))

    def product(j, xx):
        total = jnp.zeros((local, wide), f32)
        at = pl.ds(pl.multiple_of(j * wide, wide), wide)
        for zz in range(n):
            total = total + jnp.dot(got_ref[zz, xx], p_ref[zz, :, at], preferred_element_type=f32)
        return total

    def d_copy(j):
        return remote(away_ref.at[j], theirs_ref.at[j], ds.at[j], dr.at[j], (g, z, t_x))

    others(lambda zz: y_wait(zz, 1 - x).wait_recv())

    def send(j, carry):
        value = product(j, 1 - x).astype(bf16)

        @pl.when(j > 0)
        def _():
            d_copy(j - 1).start()

        away_ref[j] = value
        return carry

    lax.fori_loop(0, steps, send, 0)
    others(lambda zz: y_wait(zz, x).wait_recv())
    d_copy(steps - 1).start()

    def keep(j, carry):
        mine_ref[j] = product(j, x)
        return carry

    lax.fori_loop(0, steps, keep, 0)
    for j in range(steps):
        d_copy(j).wait_recv()
        out_ref[:, j * wide:(j + 1) * wide] = (mine_ref[j] + theirs_ref[j].astype(f32)).astype(bf16)
    for j in range(steps):
        d_copy(j).wait_send()
    for xx in (1 - x, x):
        others(lambda zz: y_copy_to(zz, xx).wait_send())

    def drain(here):
        for way in range(2):
            if (here < n - 1) if way == 0 else (here > 0):
                w_each(here, way, lambda copy: copy.wait_send())
                for zz in (range(here + 1) if way == 0 else range(here, n)):
                    for h in range(CHUNKS):
                        z_copy(zz, h, way, here).wait_send()
        own_each(here, None, lambda copy: copy.wait_send())

    for here in range(n):
        pl.when(z == here)(functools.partial(drain, here))

    def finished(zz, carry):
        for h in range(CHUNKS):
            x_copy(zz, h).wait_send()
            for xx in range(2):
                c_copy(zz, xx, h).wait_send()

        @pl.when(zz != z)
        def _():
            for m in range(MATS):
                y_copy(zz, m).wait_send()

        for copy in r_copies(zz):
            copy.wait_send()
        return carry

    lax.fori_loop(0, n, finished, 0)


def whole(
    n, tokens, norm_gain, query_diff, query_win, key_diff, value_diff, keyval_win, proj_diff, proj_win, scal,
    output_norm_gain,
):
    local, width = tokens.shape
    held = n // 2
    dma = pltpu.SemaphoreType.DMA
    inside = pl.BlockSpec(memory_space=pltpu.VMEM)
    far = pl.BlockSpec(memory_space=pl.ANY)
    cols = MATS * LANES
    tok = 4 * local * n
    feats = VDIM + 2 * HEAD
    steps = 8
    quad = 4 * local // CHUNKS
    bf16, f32 = jnp.bfloat16, jnp.float32
    return pl.pallas_call(
        functools.partial(whole_kernel, n, held),
        in_specs=[inside, inside] + [far] * 7 + [inside, inside],
        out_specs=inside,
        out_shape=jax.ShapeDtypeStruct((local, width), bf16),
        scratch_shapes=[
            pltpu.VMEM((n, CHUNKS, quad, width), bf16),
            pltpu.VMEM((width, cols), bf16),
            pltpu.VMEM((n, 4 * local, cols), f32),
            pltpu.VMEM((2, n, CHUNKS, quad, cols), bf16),
            pltpu.VMEM((2,) + scal.shape, f32),
            pltpu.VMEM((n, feats, width), bf16),
            pltpu.VMEM((tok, VDIM), bf16),
            pltpu.VMEM((n, 2, local, feats), bf16),
            pltpu.VMEM((n, 2, local, feats), bf16),
            pltpu.VMEM((steps, local, width // steps), f32),
            pltpu.VMEM((steps, local, width // steps), bf16),
            pltpu.VMEM((steps, local, width // steps), bf16),
            dma((2, n, CHUNKS)), dma((2, n + 1, CHUNKS)),
            dma((n, CHUNKS)), dma((n, CHUNKS)),
            dma((n, 2, CHUNKS)), dma((n, 2, CHUNKS)),
            dma((held, 2, MATS)), dma((n, MATS)),
            dma((n, MATS)), dma((n, MATS)), dma((MATS,)),
            dma((n, 3)), dma((n, 3)),
            dma((held, 2)), dma((held, 2)), dma((held, 2)), dma, dma,
            dma((n, 2)), dma((n, 2)), dma((steps,)), dma((steps,)),
        ],
        compiler_params=pltpu.CompilerParams(
            collective_id=0, has_side_effects=True, vmem_limit_bytes=67043328
        ),
        cost_estimate=pl.CostEstimate(
            flops=2 * tok * width * cols, bytes_accessed=2 * width * (tok + cols), transcendentals=0
        ),
    )(
        tokens, norm_gain.reshape(1, width), query_diff, query_win, key_diff, value_diff, keyval_win,
        proj_diff, proj_win, scal, output_norm_gain.reshape(1, VDIM),
    )


def split_body(
    tokens, norm_gain, query_diff, key_diff, value_diff, lam, output_norm_gain,
    query_win, keyval_win, sink, proj_diff, proj_win,
):
    n = lax.axis_size("sp")
    scal = jnp.stack([jnp.pad(lam, (0, LANES - lam.shape[0])), jnp.pad(sink, (0, LANES - sink.shape[0]))])
    scal = jnp.pad(scal, ((0, 6), (0, 0)))
    return whole(
        n, tokens, norm_gain, query_diff, query_win, key_diff, value_diff, keyval_win, proj_diff, proj_win, scal,
        output_norm_gain,
    )


def splits(mesh, tokens, query_diff, query_win, lam, sink):
    parts, n, tp = (mesh.shape[a] for a in ("grp", "sp", "tp"))
    return (
        parts == 2 and tp == 4 and n % 2 == 0
        and lam.shape[0] == 2 * n and sink.shape[0] == 2 * lam.shape[0]
        and tokens.shape[0] == parts * n * tp * WINDOW
        and query_diff.shape[1] == lam.shape[0] * 2 * HEAD and VDIM == 2 * HEAD
        and query_win.shape[1] == sink.shape[0] * HEAD and HEAD == LANES
    )


def solution(mesh):
    placed = (
        P(("grp", "sp", "tp"), None),
        P(),
        P("sp", "tp"),
        P("sp", "tp"),
        P("sp", "tp"),
        P("tp"),
        P(),
        P("sp", "tp"),
        P(None, "sp", None),
        P("tp"),
        P("tp", None),
        P("tp", None),
    )

    def build(body):
        return jax.shard_map(
            body, mesh=mesh, in_specs=placed, out_specs=P(("grp", "sp", "tp"), None), check_vma=False
        )

    general = build(general_body)

    def step(*args):
        tokens, query_diff, lam, query_win, sink = (args[i] for i in (0, 2, 5, 7, 9))
        if splits(mesh, tokens, query_diff, query_win, lam, sink):
            return build(split_body)(*args)
        return general(*args)

    return step
```

```python
import functools
import math

import jax
import jax.numpy as jnp
from jax import lax
from jax.experimental import pallas as pl
from jax.experimental.pallas import tpu as pltpu
from jax.sharding import PartitionSpec as P


HEAD = 128
WIN_HEADS = 16
KV_HEADS = 4
WINDOW = 128
VDIM = 256


EPS = 1e-06


def padded_2(x, sides, width):
    for axis, dim in sides:
        devices, length = (lax.axis_size(axis), x.shape[dim])
        up = [(i, (i + 1) % devices) for i in range(devices - 1)]
        down = [(j, i) for i, j in up]
        last = lax.slice_in_dim(x, length - width, length, axis=dim)
        first = lax.slice_in_dim(x, 0, width, axis=dim)
        before = lax.ppermute(last, axis, up)
        after = lax.ppermute(first, axis, down)
        x = jnp.concatenate([before, x, after], axis=dim)
    return x


def root_mean_square_rows(values, gain):
    return values * lax.rsqrt(jnp.mean(values * values, axis=-1, keepdims=True) + EPS) * gain


def shifted(x, axis, by):
    n = lax.axis_size(axis)
    return lax.ppermute(x, axis, [(i, (i + by) % n) for i in range(n)])


def shift_chip(x, by):
    n = lax.axis_size("tp")
    return lax.ppermute(x, "tp", [(i, (i + 2 * by) % n) for i in range(n)])


def swap_core(x):
    n = lax.axis_size("tp")
    return lax.ppermute(x, "tp", [(i, i ^ 1) for i in range(n)])


def gather_tp(x, axis):
    tp = lax.axis_size("tp")
    chips = tp // 2
    me = lax.axis_index("tp")
    mine = [x] + [shift_chip(x, r) for r in range(1, chips)]
    theirs = [swap_core(piece) for piece in mine]
    out = jnp.zeros(x.shape[:axis] + (tp,) + x.shape[axis:], x.dtype)
    for r in range(chips):
        at = (me - 2 * r) % tp
        out = lax.dynamic_update_slice_in_dim(out, jnp.expand_dims(mine[r], axis), at, axis)
        out = lax.dynamic_update_slice_in_dim(out, jnp.expand_dims(theirs[r], axis), at ^ 1, axis)
    return out


def scatter_tp(x):
    tp = lax.axis_size("tp")
    chips = tp // 2
    me = lax.axis_index("tp")
    core, chip = me % 2, me // 2
    x = x.reshape(chips, 2, x.shape[0] // tp, x.shape[1])
    away = lax.dynamic_index_in_dim(x, 1 - core, 1, keepdims=False).astype(jnp.bfloat16)
    keep = lax.dynamic_index_in_dim(x, core, 1, keepdims=False)
    both = keep + swap_core(away).astype(jnp.float32)
    total = lax.dynamic_index_in_dim(both, chip, 0, keepdims=False)
    for r in range(1, chips):
        sent = lax.dynamic_index_in_dim(both, (chip + r) % chips, 0, keepdims=False)
        total = total + shift_chip(sent.astype(jnp.bfloat16), r).astype(jnp.float32)
    return total.astype(jnp.bfloat16)


def diff_kernel(lam_ref, q_ref, k_ref, v_ref, gain_ref, o_ref):
    factor = HEAD ** (-0.5) * math.log2(math.e)
    maps = []
    for m in range(2):
        cols = slice(m * HEAD, (m + 1) * HEAD)
        scores = lax.dot_general(
            q_ref[:, cols], k_ref[:, cols], (((1,), (1,)), ((), ())),
            preferred_element_type=jnp.float32,
        )
        top = jnp.max(scores, axis=-1, keepdims=True)
        expo = jnp.exp2((scores - top) * factor)
        total = jnp.sum(expo, axis=-1, keepdims=True)
        out = jnp.dot(expo.astype(jnp.bfloat16), v_ref[...], preferred_element_type=jnp.float32)
        maps.append(out / total)
    d = maps[0] - lam_ref[pl.program_id(0)] * maps[1]
    d = d * lax.rsqrt(jnp.mean(d * d, axis=-1, keepdims=True) + EPS) * gain_ref[...]
    o_ref[...] = d.astype(jnp.bfloat16)


def diff_attention(q, kv, lam, gain):
    tok, rows, heads = q.shape[0], kv.shape[0], lam.shape[0]
    tile = math.gcd(tok, max(128, 524288 // rows))
    return pl.pallas_call(
        diff_kernel,
        grid=(heads, tok // tile),
        in_specs=[
            pl.BlockSpec(memory_space=pltpu.SMEM),
            pl.BlockSpec((tile, 2 * HEAD), lambda h, i: (i, h)),
            pl.BlockSpec((rows, 2 * HEAD), lambda h, i: (0, h)),
            pl.BlockSpec((rows, VDIM), lambda h, i: (0, heads + h)),
            pl.BlockSpec((1, VDIM), lambda h, i: (0, 0)),
        ],
        out_specs=pl.BlockSpec((tile, VDIM), lambda h, i: (i, h)),
        out_shape=jax.ShapeDtypeStruct((tok, heads * VDIM), jnp.bfloat16),
        cost_estimate=pl.CostEstimate(
            flops=heads * tok * rows * 2 * 2 * (HEAD + VDIM),
            bytes_accessed=2 * (q.size * 2 + kv.size),
            transcendentals=heads * 2 * tok * rows,
        ),
    )(lam, q, kv, kv, gain.reshape(1, VDIM))


def general_body(
    tokens,
    norm_gain,
    query_diff,
    key_diff,
    value_diff,
    lam,
    output_norm_gain,
    query_win,
    keyval_win,
    sink,
    proj_diff,
    proj_win,
):
    bf16, f32 = jnp.bfloat16, jnp.float32
    normed = root_mean_square_rows(tokens.astype(f32), norm_gain).astype(bf16)
    heads_win = sink.shape[0]
    group = WIN_HEADS // KV_HEADS
    n = lax.axis_size("sp")
    me = lax.axis_index("sp")
    parts = lax.axis_size("grp")
    part = lax.axis_index("grp")
    local, width = normed.shape
    depth = width // n
    tok = local * lax.axis_size("tp")

    slabs = normed.reshape(local, n, depth)
    across = jnp.zeros((n, local, depth), bf16)
    own = lax.dynamic_index_in_dim(slabs, me, 1, keepdims=True)
    across = lax.dynamic_update_slice_in_dim(across, jnp.swapaxes(own, 0, 1), me, 0)
    for r in range(1, n):
        sent = lax.dynamic_index_in_dim(slabs, (me + r) % n, 1, keepdims=False)
        got = shifted(sent, "sp", r)
        across = lax.dynamic_update_slice_in_dim(across, got[None], (me - r) % n, 0)

    kv_index = lax.axis_index("tp") * heads_win // group
    kv_local = lax.dynamic_index_in_dim(keyval_win, kv_index, 0, keepdims=False)
    stacked = jnp.concatenate([query_diff, query_win, kv_local], axis=1)
    share = stacked.shape[1] // parts
    half = lax.dynamic_slice_in_dim(stacked, part * share, share, axis=1)
    across, half = lax.optimization_barrier((across, half))

    pieces = [shifted(half, "sp", r) for r in range(1, n)]
    all_rows = gather_tp(across, 1).reshape(n * tok, depth)
    rows_all = gather_tp(normed, 0).reshape(tok, width)
    kv_part = jnp.concatenate(
        [
            jnp.dot(all_rows, key_diff, preferred_element_type=f32).astype(bf16),
            jnp.dot(all_rows, value_diff, preferred_element_type=f32).astype(bf16),
        ],
        axis=1,
    )
    kv = lax.psum_scatter(kv_part, "sp", scatter_dimension=0, tiled=True)
    kv = lax.all_gather(kv, "sp", axis=0, tiled=True)

    own_rows = lax.dynamic_slice_in_dim(rows_all, me * depth, depth, axis=1)
    own_sum = jnp.dot(own_rows, stacked, preferred_element_type=f32)
    sums = [jnp.zeros((tok, share), f32) for _ in range(parts)]
    for r in range(1, n):
        piece = pieces[r - 1]
        rows = lax.dynamic_slice_in_dim(rows_all, (me - r) % n * depth, depth, axis=1)
        for j in range(parts):
            block = piece if j == 0 else shifted(piece, "grp", j)
            sums[j] = sums[j] + jnp.dot(rows, block, preferred_element_type=f32)
    ordered = jnp.stack(sums)
    ordered = jnp.concatenate(
        [
            lax.dynamic_index_in_dim(ordered, (part - b) % parts, 0, keepdims=False)
            for b in range(parts)
        ],
        axis=1,
    )
    projected = (own_sum + ordered).astype(bf16)
    first = query_diff.shape[1]
    second = first + query_win.shape[1]
    q_diff, q_win, kv_win = projected[:, :first], projected[:, first:second], projected[:, second:]
    scale = HEAD ** (-0.5)
    padded = padded_2(kv_win, (("sp", 0),), WINDOW)
    nblocks = tok // WINDOW
    blocks = padded.reshape(nblocks + 2, WINDOW, 2 * HEAD)
    band = jnp.concatenate([blocks[:-2], blocks[1:-1], blocks[2:]], axis=1)
    q_blocks = q_win.reshape(nblocks, WINDOW, heads_win, HEAD)
    scores = (
        jnp.einsum("nqhd,nkd->nhqk", q_blocks, band[..., :HEAD], preferred_element_type=jnp.float32)
        * scale
    )
    q_index = jnp.arange(WINDOW)
    k_index = jnp.arange(3 * WINDOW)
    relative = k_index[None, :] - WINDOW - q_index[:, None]
    first_key = lax.axis_index("sp") * tok - WINDOW
    key_pos = first_key + jnp.arange(nblocks)[:, None] * WINDOW + k_index[None, :]
    inside = (key_pos >= 0) & (key_pos < tok * lax.axis_size("sp"))
    valid = (jnp.abs(relative) <= WINDOW)[None] & inside[:, None, :]
    scores = jnp.where(valid[:, None], scores, -jnp.inf)
    sink_logit = sink[None, :, None, None]
    top_win = jnp.maximum(jnp.max(scores, axis=-1, keepdims=True), sink_logit)
    expo = jnp.exp(scores - top_win)
    weights = expo / (jnp.sum(expo, axis=-1, keepdims=True) + jnp.exp(sink_logit - top_win))
    y_win = jnp.einsum(
        "nhqk,nkd->nqhd",
        weights.astype(jnp.bfloat16),
        band[..., HEAD:],
        preferred_element_type=jnp.float32,
    ).astype(jnp.bfloat16)
    y_win = y_win.reshape(tok, heads_win * HEAD)
    summed = jnp.dot(y_win, proj_win, preferred_element_type=jnp.float32)
    differential_output = diff_attention(q_diff, kv, lam, output_norm_gain)
    summed = summed + jnp.dot(differential_output, proj_diff, preferred_element_type=jnp.float32)
    return scatter_tp(summed)


MESH = pl.DeviceIdType.MESH
CHUNKS = 4
LANES = 128
MATS = 5


def remote(src, dst, send, recv, device):
    return pltpu.make_async_remote_copy(
        src_ref=src, dst_ref=dst, send_sem=send, recv_sem=recv, device_id=device, device_id_type=MESH
    )


def place():
    g, z, t = lax.axis_index("grp"), lax.axis_index("sp"), lax.axis_index("tp")
    x, c = t // 2, t % 2
    return g, z, t, x, c, 2 * (1 - x) + c, 2 * x + 1 - c


def greet(devices, meanwhile):
    barrier = pltpu.get_barrier_semaphore()
    for device in devices:
        pl.semaphore_signal(barrier, inc=1, device_id=device, device_id_type=MESH)
    meanwhile()
    pl.semaphore_wait(barrier, len(devices))


def arrivals(n, here):
    times = []
    for k in range(1, n):
        for h in range(CHUNKS):
            at = k - 1 + (h + 1) / CHUNKS
            if here - k >= 0:
                times.append((at, "z", here - k, h, 0, k))
            if here + k < n:
                times.append((at + 0.01, "z", here + k, h, 1, k))
    times.sort()
    clock = 0.0
    beside = []
    for at, zz, h in [(0.0, here, h) for h in range(CHUNKS)] + [(e[0], e[2], e[3]) for e in times]:
        clock = max(clock, at) + 1 / CHUNKS
        beside.append((clock + 0.05, "x", zz, h, 0, 0))
    return times + beside


def order(n, here):
    def start(zz):
        return (zz + 1 if zz < here else n - zz, abs(zz - here))

    return sorted((zz for zz in range(n) if zz != here), key=start)


def whole_kernel(
    n, held, tok_hbm, gain_hbm, qd, qw, kd, vd, kvw, pd, pw, lam_ref, sink_ref, out_gain_ref,
    out_ref,
    tok_ref, gain_ref, scal_ref, enter, rows_ref, w_ref, sum_ref, res_ref, oscal_ref, p_ref, v_ref, y_ref, got_ref, mine_ref, away_ref, theirs_ref,
    zs, zr, xs, xr, cs, cr, ws, wr, ys, yr, own_sem, rs, rr, ps, pr, load, scal_s, scal_r, hs, hr, ds, dr,
):
    g, z, t, x, c, t_x, t_c = place()
    local, width = tok_hbm.shape
    part = local // CHUNKS
    depth = qd.shape[0]
    half = depth // 2
    group = WIN_HEADS // KV_HEADS
    mats = (qd, qw, kd, vd, kvw)
    core = (g, z, t_c)
    f32, bf16 = jnp.float32, jnp.bfloat16

    def block(zz, h, tt):
        return rows_ref.at[zz, h, pl.ds(pl.multiple_of(tt * part, part), part)]

    entries = [pltpu.make_async_copy(tok_hbm, tok_ref, enter.at[0]), pltpu.make_async_copy(gain_hbm, gain_ref, enter.at[1])]
    for copy in entries:
        copy.start()

    def normalize():
        scal_ref[...] = jnp.zeros(scal_ref.shape, f32)
        scal_ref[0:1, 0:held] = lam_ref[...]
        scal_ref[1:2, 0:2 * held] = sink_ref[...]
        oscal_ref[c] = scal_ref[...]
        for copy in entries:
            copy.wait()
        for h in range(CHUNKS):
            v = tok_ref[h * part:(h + 1) * part, :].astype(f32)
            v = v * lax.rsqrt(jnp.mean(v * v, axis=-1, keepdims=True) + EPS) * gain_ref[...]
            rows_ref[z, h, pl.ds(pl.multiple_of(t * part, part), part), :] = v.astype(bf16)

    greet(
        [(g, lax.rem(z + i // 2, n), 2 * x + (c + i % 2) % 2) for i in range(1, 2 * n)]
        + [(g, z, t_x), (1 - g, z, t)],
        normalize,
    )

    def w_half(zz, yy, m):
        at = pl.ds(pl.multiple_of(zz * depth + yy * half, half), half)
        return w_ref.at[at, m * LANES:(m + 1) * LANES]

    def source(dz, i, cc, m, at):
        if m == MATS - 1:
            return kvw.at[(2 * (x * n + dz)) // group, at, cc * LANES:(cc + 1) * LANES]
        return mats[m].at[at, (2 * i + cc) * LANES:(2 * i + cc + 1) * LANES]

    def w_copy(here, dz, cc, m):
        at = pl.ds(pl.multiple_of(g * half, half), half)
        return remote(
            source(dz, dz % held, cc, m, at), w_half(here, g, m),
            ws.at[dz % held, cc, m], wr.at[here, m], (g, dz, 2 * x + cc),
        )

    def w_each(here, way, act):
        for cs_ in range(2):
            @pl.when(c == cs_)
            def _():
                for m in range(MATS):
                    for dz in range(cs_ * held, (cs_ + 1) * held):
                        if (dz > here) if way == 0 else (dz < here):
                            for cc in range(2):
                                act(w_copy(here, dz, cc, m))

    def own_copy(here, cc, m):
        at = pl.ds(0, depth)
        target = w_ref.at[here * depth:(here + 1) * depth, m * LANES:(m + 1) * LANES]
        return source(here, here % held, cc, m, at), target

    def own_each(here, near, away):
        for cc in range(2):
            for m in range(MATS):
                a, b = own_copy(here, cc, m)

                if near is not None:
                    @pl.when((c == here // held) & (c == cc))
                    def _():
                        near(pltpu.make_async_copy(a, b, own_sem.at[m]))

                @pl.when((c == here // held) & (c != cc))
                def _():
                    away(remote(a, b, ws.at[here % held, cc, m], own_sem.at[m], core))

    def z_copy(zz, h, way, here):
        k = abs(zz - here)
        to = here + 1 if way == 0 else here - 1
        return remote(block(zz, h, t), block(zz, h, t), zs.at[way, k, h], zr.at[way, k + 1, h], (g, to, t))

    def x_copy(zz, h):
        return remote(block(zz, h, t), block(zz, h, t), xs.at[zz, h], xr.at[zz, h], (g, z, t_x))

    def c_copy(zz, xx, h):
        tt = 2 * xx + c
        return remote(block(zz, h, tt), block(zz, h, tt), cs.at[zz, xx, h], cr.at[zz, xx, h], core)

    def y_copy(zz, m):
        return remote(w_half(zz, g, m), w_half(zz, g, m), ys.at[zz, m], yr.at[zz, m], (1 - g, z, t))

    def forward(zz, m):
        remote(w_half(zz, g, m), w_half(zz, g, m), ys.at[zz, m], wr.at[zz, m], core).wait_recv()
        y_copy(zz, m).start()

    def crossed(zz):
        for m in range(MATS):
            remote(w_half(zz, 1 - g, m), w_half(zz, 1 - g, m), ys.at[zz, m], yr.at[zz, m], core).wait_recv()

    scal_copy = remote(scal_ref, oscal_ref.at[c], scal_s, scal_r, core)

    def gather(here):
        for h in range(CHUNKS):
            if here < n - 1:
                z_copy(here, h, 0, here).start()
            if here > 0:
                z_copy(here, h, 1, here).start()
            x_copy(here, h).start()
            c_copy(here, x, h).start()
        scal_copy.start()
        own_each(here, lambda copy: copy.start(), lambda copy: copy.start())
        if here == 0:
            w_each(here, 0, lambda copy: copy.start())
        if here == n - 1:
            w_each(here, 1, lambda copy: copy.start())
        first = order(n, here)[0]
        begin = first + 1 if first < here else n - first
        events = arrivals(n, here)
        events += [(begin + 0.5 * (m + 1), "w", first, m, 0, 0) for m in range(MATS)]
        for at, kind, zz, h, way, k in sorted(events):
            if kind == "z":
                remote(block(zz, h, t), block(zz, h, t), zs.at[way, k, h], zr.at[way, k, h], core).wait_recv()
                if (here < n - 1) if way == 0 else (here > 0):
                    z_copy(zz, h, way, here).start()
                x_copy(zz, h).start()
                c_copy(zz, x, h).start()
                if h == CHUNKS - 1 and zz == (0 if way == 0 else n - 1):
                    w_each(here, way, lambda copy: copy.start())
            elif kind == "x":
                x_copy(zz, h).wait_recv()
                c_copy(zz, 1 - x, h).start()
            else:
                forward(zz, h)

    for here in range(n):
        pl.when(z == here)(functools.partial(gather, here))

    proj_copies, loads = [], []
    for i in range(held):
        for j, ref in enumerate((pd, pw)):
            rows = ref.at[i * VDIM:(i + 1) * VDIM]
            at = p_ref.at[c * held + i, j * VDIM:(j + 1) * VDIM]
            loads.append(pltpu.make_async_copy(rows, at, load.at[i, j]))
            proj_copies.append(remote(rows, at, ps.at[i, j], pr.at[i, j], core))
    for copy in loads + proj_copies:
        copy.start()

    sources = []
    for j in range(n - 1):
        zz = order(n, 0)[j] + 0 * z
        for here in range(1, n):
            zz = jnp.where(z == here, order(n, here)[j], zz)
        sources.append(zz)

    quad = rows_ref.shape[2]

    def partial_sum(zz, at, size):
        k = pl.ds(pl.multiple_of(at, half), size)
        left = rows_ref[zz, :, :, k].reshape(CHUNKS * quad, size)
        return jnp.dot(left, w_ref[k, :], preferred_element_type=f32)

    def opening(zz, carry):
        for xx in range(2):
            for h in range(CHUNKS):
                c_copy(zz, xx, h).wait_recv()
        sum_ref[zz] = partial_sum(zz, z * depth, depth)
        return carry

    def add(at):
        def one(zz, carry):
            sum_ref[zz] += partial_sum(zz, at, half)
            return carry

        lax.fori_loop(0, n, one, 0)

    def r_copies(zz):
        copies = [remote(
            res_ref.at[c, zz, :, :, 2 * LANES:], res_ref.at[c, zz, :, :, 2 * LANES:],
            rs.at[zz, 0], rr.at[zz, 0], core,
        )]
        for xx in range(2):
            at = pl.ds(pl.multiple_of((2 * xx + 1 - c) * part, part), part)
            copies.append(remote(
                res_ref.at[c, zz, :, at, :2 * LANES], res_ref.at[c, zz, :, at, :2 * LANES],
                rs.at[zz, 1 + xx], rr.at[zz, 1 + xx], core,
            ))
        return copies

    for m in range(MATS):
        a, b = own_copy(0, 0, m)
        pltpu.make_async_copy(a, b, own_sem.at[m]).wait()
    late = sources[1:]

    def forwards(lo, hi):
        for m in range(lo, hi):
            for zz in late:
                forward(zz, m)

    forwards(0, 1)
    lax.fori_loop(0, n, opening, 0)
    forwards(1, 2)
    add(sources[0] * depth + g * half)
    crossed(sources[0])
    add(sources[0] * depth + (1 - g) * half)
    forwards(2, MATS)
    for zz in late:
        add(zz * depth + g * half)
    for zz in late[:-1]:
        crossed(zz)
        add(zz * depth + (1 - g) * half)
    crossed(sources[-1])

    def closing(zz, carry):
        total = sum_ref[zz] + partial_sum(zz, sources[-1] * depth + (1 - g) * half, half)

        @pl.when(zz > 0)
        def _():
            for copy in r_copies(zz - 1):
                copy.start()

        res_ref[c, zz] = total.astype(bf16).reshape(CHUNKS, quad, MATS * LANES)
        return carry

    lax.fori_loop(0, n, closing, 0)
    scal_copy.wait()
    for copy in r_copies(n - 1):
        copy.start()

    def exchanged(zz, carry):
        for copy in r_copies(zz):
            copy.wait_recv()
        return carry

    lax.fori_loop(0, n, exchanged, 0)

    rows = n * 4 * local
    factor = HEAD ** (-0.5) * math.log2(math.e)
    for i in range(2):
        v_ref[:, i * LANES:(i + 1) * LANES] = res_ref[i, :, :, :, 3 * LANES:4 * LANES].reshape(rows, LANES)

    level = oscal_ref[z // held]
    level_row = lax.broadcasted_iota(jnp.int32, level.shape, 0)
    level_lane = lax.broadcasted_iota(jnp.int32, level.shape, 1)

    def scalar(row, lane):
        picked = jnp.where((level_row == row) & (level_lane == lane), level, 0.0)
        return jnp.sum(jnp.sum(picked, axis=1, keepdims=True), axis=0, keepdims=True)

    lam = scalar(0, z % held)
    sinks = [scalar(1, 2 * (z % held) + i) for i in range(2)]
    first = lax.broadcasted_iota(jnp.int32, (local, 1), 0) < local // 2
    sink = jnp.where(first, sinks[0], sinks[1])

    distant = []
    for j in range(n):
        zz = 0 * z
        for here in range(n):
            far = sorted(range(n), key=lambda o: -abs(o - here))[j]
            zz = jnp.where(z == here, far, zz)
        distant.append(zz)

    fine = local // 2
    some = CHUNKS // 2

    def piece(i, zz, tt, m, e=None):
        at = pl.ds(pl.multiple_of(tt * part, part), part)
        if e is None:
            return res_ref[i, zz, :, at, m * LANES:(m + 1) * LANES].reshape(local, LANES)
        return res_ref[i, zz, pl.ds(e * some, some), at, m * LANES:(m + 1) * LANES].reshape(fine, LANES)

    def rows_of(e):
        return pl.ds(pl.multiple_of(e * fine, fine), fine)

    def y_copy_to(zz, xx, e):
        return remote(
            y_ref.at[zz, xx, rows_of(e)], got_ref.at[z, xx, rows_of(e)],
            hs.at[zz, xx, e], hr.at[z, xx, e], (g, zz, t),
        )

    def y_wait(zz, xx, e):
        rows = got_ref.at[zz, xx, rows_of(e)]
        return remote(rows, rows, hs.at[zz, xx, e], hr.at[zz, xx, e], (g, z, t_x))

    def windowed(zz, tt, xx, e):
        b = 4 * zz + tt

        def banded(i):
            pieces = []
            for o in (-1, 0, 1):
                o = jnp.clip(b + o, 0, 4 * n - 1)
                pieces.append(piece(i, o // 4, o % 4, 4))
            return jnp.concatenate(pieces, axis=0)

        q = jnp.concatenate([piece(i, zz, tt, 1, e) for i in range(2)], axis=0)
        scores = lax.dot_general(
            q, banded(0), (((1,), (1,)), ((), ())), preferred_element_type=f32
        ) * HEAD ** (-0.5)
        r_index = lax.broadcasted_iota(jnp.int32, scores.shape, 0) % fine + e * fine
        k_index = lax.broadcasted_iota(jnp.int32, scores.shape, 1)
        spot = (b - 1) * local + k_index
        valid = (jnp.abs(k_index - local - r_index) <= WINDOW) & (spot >= 0) & (spot < rows)
        scores = jnp.where(valid, scores, -jnp.inf)
        top = jnp.maximum(jnp.max(scores, axis=-1, keepdims=True), sink)
        expo = jnp.exp(scores - top)
        weights = expo / (jnp.sum(expo, axis=-1, keepdims=True) + jnp.exp(sink - top))
        out = jnp.dot(weights.astype(bf16), banded(1), preferred_element_type=f32).astype(bf16)
        for i in range(2):
            y_ref[zz, xx, rows_of(e), VDIM + i * LANES:VDIM + (i + 1) * LANES] = out[i * fine:(i + 1) * fine]

    def attend(step):
        xx = jnp.where(step < 2, 1 - x, x)
        tt = 2 * xx + c
        e = step % 2
        maps = []
        for m in range(2):
            q = jnp.concatenate([piece(m, zz, tt, 0, e) for zz in distant], axis=0)
            keys = res_ref[m, :, :, :, 2 * LANES:3 * LANES].reshape(rows, LANES)
            scores = lax.dot_general(q, keys, (((1,), (1,)), ((), ())), preferred_element_type=f32)
            top = jnp.max(scores, axis=-1, keepdims=True)
            expo = jnp.exp2((scores - top) * factor)
            total = jnp.sum(expo, axis=-1, keepdims=True)
            out = jnp.dot(expo.astype(bf16), v_ref[...], preferred_element_type=f32)
            maps.append(out / total)
        d = maps[0] - lam * maps[1]
        d = d * lax.rsqrt(jnp.mean(d * d, axis=-1, keepdims=True) + EPS) * out_gain_ref[...]
        d = d.astype(bf16)
        for i, zz in enumerate(distant):
            y_ref[zz, xx, rows_of(e), :VDIM] = d[i * fine:(i + 1) * fine]
        for zz in distant:
            windowed(zz, tt, xx, e)
        for zz in distant:
            @pl.when(zz != z)
            def _():
                y_copy_to(zz, xx, e).start()
        got_ref[z, xx, rows_of(e)] = y_ref[z, xx, rows_of(e)]

    steps = mine_ref.shape[1]
    wide = width // steps

    def others(act):
        for d in range(n - 1, 0, -1):
            pl.when(z - d >= 0)(functools.partial(act, z - d))
            pl.when(z + d < n)(functools.partial(act, z + d))

    def product(j, xx, e):
        total = jnp.zeros((fine, wide), f32)
        at = pl.ds(pl.multiple_of(j * wide, wide), wide)
        for zz in range(n):
            total = total + jnp.dot(
                got_ref[zz, xx, rows_of(e)], p_ref[zz, :, at], preferred_element_type=f32
            )
        return total

    def d_copy(e, j):
        return remote(away_ref.at[e, j], theirs_ref.at[e, j], ds.at[e, j], dr.at[e, j], (g, z, t_x))

    def send_rows(e):
        @pl.when(e == 0)
        def _():
            for copy in loads + proj_copies:
                copy.wait()

        others(lambda zz: y_wait(zz, 1 - x, e).wait_recv())

        def send(j, carry):
            value = product(j, 1 - x, e).astype(bf16)

            @pl.when(j > 0)
            def _():
                d_copy(e, j - 1).start()

            away_ref[e, j] = value
            return carry

        lax.fori_loop(0, steps, send, 0)
        d_copy(e, steps - 1).start()

    def stage(step, carry):
        attend(step)
        pl.when((step >= 1) & (step <= 2))(lambda: send_rows(step - 1))
        return carry

    lax.fori_loop(0, 4, stage, 0)

    def keep_rows(e, carry):
        others(lambda zz: y_wait(zz, x, e).wait_recv())

        def keep(j, carry):
            mine_ref[e, j] = product(j, x, e)
            return carry

        lax.fori_loop(0, steps, keep, 0)
        return carry

    lax.fori_loop(0, 2, keep_rows, 0)
    for e in range(2):
        for j in range(steps):
            d_copy(e, j).wait_recv()
            total = mine_ref[e, j] + theirs_ref[e, j].astype(f32)
            out_ref[e * fine:(e + 1) * fine, j * wide:(j + 1) * wide] = total.astype(bf16)
    for e in range(2):
        for j in range(steps):
            d_copy(e, j).wait_send()
        for xx in (1 - x, x):
            others(lambda zz: y_copy_to(zz, xx, e).wait_send())

    def drain(here):
        for way in range(2):
            if (here < n - 1) if way == 0 else (here > 0):
                w_each(here, way, lambda copy: copy.wait_send())
                for zz in (range(here + 1) if way == 0 else range(here, n)):
                    for h in range(CHUNKS):
                        z_copy(zz, h, way, here).wait_send()
        own_each(here, None, lambda copy: copy.wait_send())

    for here in range(n):
        pl.when(z == here)(functools.partial(drain, here))

    def finished(zz, carry):
        for h in range(CHUNKS):
            x_copy(zz, h).wait_send()
            for xx in range(2):
                c_copy(zz, xx, h).wait_send()

        @pl.when(zz != z)
        def _():
            for m in range(MATS):
                y_copy(zz, m).wait_send()

        for copy in r_copies(zz):
            copy.wait_send()
        return carry

    lax.fori_loop(0, n, finished, 0)


def whole(
    n, tokens, norm_gain, query_diff, query_win, key_diff, value_diff, keyval_win, proj_diff, proj_win, lam, sink,
    output_norm_gain,
):
    local, width = tokens.shape
    held = n // 2
    dma = pltpu.SemaphoreType.DMA
    inside = pl.BlockSpec(memory_space=pltpu.VMEM)
    far = pl.BlockSpec(memory_space=pl.ANY)
    cols = MATS * LANES
    tok = 4 * local * n
    feats = VDIM + 2 * HEAD
    steps = 4
    quad = 4 * local // CHUNKS
    bf16, f32 = jnp.bfloat16, jnp.float32
    return pl.pallas_call(
        functools.partial(whole_kernel, n, held),
        in_specs=[far] * 9 + [inside] * 3,
        out_specs=inside,
        out_shape=jax.ShapeDtypeStruct((local, width), bf16),
        scratch_shapes=[
            pltpu.VMEM((local, width), bf16),
            pltpu.VMEM((1, width), f32),
            pltpu.VMEM((8, LANES), f32),
            dma((2,)),
            pltpu.VMEM((n, CHUNKS, quad, width), bf16),
            pltpu.VMEM((width, cols), bf16),
            pltpu.VMEM((n, 4 * local, cols), f32),
            pltpu.VMEM((2, n, CHUNKS, quad, cols), bf16),
            pltpu.VMEM((2, 8, LANES), f32),
            pltpu.VMEM((n, feats, width), bf16),
            pltpu.VMEM((tok, VDIM), bf16),
            pltpu.VMEM((n, 2, local, feats), bf16),
            pltpu.VMEM((n, 2, local, feats), bf16),
            pltpu.VMEM((2, steps, local // 2, width // steps), f32),
            pltpu.VMEM((2, steps, local // 2, width // steps), bf16),
            pltpu.VMEM((2, steps, local // 2, width // steps), bf16),
            dma((2, n, CHUNKS)), dma((2, n + 1, CHUNKS)),
            dma((n, CHUNKS)), dma((n, CHUNKS)),
            dma((n, 2, CHUNKS)), dma((n, 2, CHUNKS)),
            dma((held, 2, MATS)), dma((n, MATS)),
            dma((n, MATS)), dma((n, MATS)), dma((MATS,)),
            dma((n, 3)), dma((n, 3)),
            dma((held, 2)), dma((held, 2)), dma((held, 2)), dma, dma,
            dma((n, 2, 2)), dma((n, 2, 2)), dma((2, steps)), dma((2, steps)),
        ],
        compiler_params=pltpu.CompilerParams(
            collective_id=0, has_side_effects=True, vmem_limit_bytes=67043328
        ),
        cost_estimate=pl.CostEstimate(
            flops=2 * tok * width * cols, bytes_accessed=2 * width * (tok + cols), transcendentals=0
        ),
    )(
        tokens, norm_gain.reshape(1, width), query_diff, query_win, key_diff, value_diff, keyval_win,
        proj_diff, proj_win, lam.reshape(1, -1), sink.reshape(1, -1), output_norm_gain.reshape(1, VDIM),
    )


def split_body(
    tokens, norm_gain, query_diff, key_diff, value_diff, lam, output_norm_gain,
    query_win, keyval_win, sink, proj_diff, proj_win,
):
    n = lax.axis_size("sp")
    return whole(
        n, tokens, norm_gain, query_diff, query_win, key_diff, value_diff, keyval_win, proj_diff, proj_win, lam, sink,
        output_norm_gain,
    )


def splits(mesh, tokens, query_diff, query_win, lam, sink):
    parts, n, tp = (mesh.shape[a] for a in ("grp", "sp", "tp"))
    return (
        parts == 2 and tp == 4 and n % 2 == 0
        and lam.shape[0] == 2 * n and sink.shape[0] == 2 * lam.shape[0]
        and tokens.shape[0] == parts * n * tp * WINDOW
        and query_diff.shape[1] == lam.shape[0] * 2 * HEAD and VDIM == 2 * HEAD
        and query_win.shape[1] == sink.shape[0] * HEAD and HEAD == LANES
    )


def solution(mesh):
    placed = (
        P(("grp", "sp", "tp"), None),
        P(),
        P("sp", "tp"),
        P("sp", "tp"),
        P("sp", "tp"),
        P("tp"),
        P(),
        P("sp", "tp"),
        P(None, "sp", None),
        P("tp"),
        P("tp", None),
        P("tp", None),
    )

    def build(body):
        return jax.shard_map(
            body, mesh=mesh, in_specs=placed, out_specs=P(("grp", "sp", "tp"), None), check_vma=False
        )

    general = build(general_body)

    def step(*args):
        tokens, query_diff, lam, query_win, sink = (args[i] for i in (0, 2, 5, 7, 9))
        if splits(mesh, tokens, query_diff, query_win, lam, sink):
            return build(split_body)(*args)
        return general(*args)

    return step
```

```python
import functools
import math

import jax
import jax.numpy as jnp
from jax import lax
from jax.experimental import pallas as pl
from jax.experimental.pallas import tpu as pltpu
from jax.sharding import PartitionSpec as P


HEAD = 128
WIN_HEADS = 16
KV_HEADS = 4
WINDOW = 128
VDIM = 256


EPS = 1e-06


def padded_2(x, sides, width):
    for axis, dim in sides:
        devices, length = (lax.axis_size(axis), x.shape[dim])
        up = [(i, (i + 1) % devices) for i in range(devices - 1)]
        down = [(j, i) for i, j in up]
        last = lax.slice_in_dim(x, length - width, length, axis=dim)
        first = lax.slice_in_dim(x, 0, width, axis=dim)
        before = lax.ppermute(last, axis, up)
        after = lax.ppermute(first, axis, down)
        x = jnp.concatenate([before, x, after], axis=dim)
    return x


def root_mean_square_rows(values, gain):
    return values * lax.rsqrt(jnp.mean(values * values, axis=-1, keepdims=True) + EPS) * gain


def shifted(x, axis, by):
    n = lax.axis_size(axis)
    return lax.ppermute(x, axis, [(i, (i + by) % n) for i in range(n)])


def shift_chip(x, by):
    n = lax.axis_size("tp")
    return lax.ppermute(x, "tp", [(i, (i + 2 * by) % n) for i in range(n)])


def swap_core(x):
    n = lax.axis_size("tp")
    return lax.ppermute(x, "tp", [(i, i ^ 1) for i in range(n)])


def gather_tp(x, axis):
    tp = lax.axis_size("tp")
    chips = tp // 2
    me = lax.axis_index("tp")
    mine = [x] + [shift_chip(x, r) for r in range(1, chips)]
    theirs = [swap_core(piece) for piece in mine]
    out = jnp.zeros(x.shape[:axis] + (tp,) + x.shape[axis:], x.dtype)
    for r in range(chips):
        at = (me - 2 * r) % tp
        out = lax.dynamic_update_slice_in_dim(out, jnp.expand_dims(mine[r], axis), at, axis)
        out = lax.dynamic_update_slice_in_dim(out, jnp.expand_dims(theirs[r], axis), at ^ 1, axis)
    return out


def scatter_tp(x):
    tp = lax.axis_size("tp")
    chips = tp // 2
    me = lax.axis_index("tp")
    core, chip = me % 2, me // 2
    x = x.reshape(chips, 2, x.shape[0] // tp, x.shape[1])
    away = lax.dynamic_index_in_dim(x, 1 - core, 1, keepdims=False).astype(jnp.bfloat16)
    keep = lax.dynamic_index_in_dim(x, core, 1, keepdims=False)
    both = keep + swap_core(away).astype(jnp.float32)
    total = lax.dynamic_index_in_dim(both, chip, 0, keepdims=False)
    for r in range(1, chips):
        sent = lax.dynamic_index_in_dim(both, (chip + r) % chips, 0, keepdims=False)
        total = total + shift_chip(sent.astype(jnp.bfloat16), r).astype(jnp.float32)
    return total.astype(jnp.bfloat16)


def diff_kernel(lam_ref, q_ref, k_ref, v_ref, gain_ref, o_ref):
    factor = HEAD ** (-0.5) * math.log2(math.e)
    maps = []
    for m in range(2):
        cols = slice(m * HEAD, (m + 1) * HEAD)
        scores = lax.dot_general(
            q_ref[:, cols], k_ref[:, cols], (((1,), (1,)), ((), ())),
            preferred_element_type=jnp.float32,
        )
        top = jnp.max(scores, axis=-1, keepdims=True)
        expo = jnp.exp2((scores - top) * factor)
        total = jnp.sum(expo, axis=-1, keepdims=True)
        out = jnp.dot(expo.astype(jnp.bfloat16), v_ref[...], preferred_element_type=jnp.float32)
        maps.append(out / total)
    d = maps[0] - lam_ref[pl.program_id(0)] * maps[1]
    d = d * lax.rsqrt(jnp.mean(d * d, axis=-1, keepdims=True) + EPS) * gain_ref[...]
    o_ref[...] = d.astype(jnp.bfloat16)


def diff_attention(q, kv, lam, gain):
    tok, rows, heads = q.shape[0], kv.shape[0], lam.shape[0]
    tile = math.gcd(tok, max(128, 524288 // rows))
    return pl.pallas_call(
        diff_kernel,
        grid=(heads, tok // tile),
        in_specs=[
            pl.BlockSpec(memory_space=pltpu.SMEM),
            pl.BlockSpec((tile, 2 * HEAD), lambda h, i: (i, h)),
            pl.BlockSpec((rows, 2 * HEAD), lambda h, i: (0, h)),
            pl.BlockSpec((rows, VDIM), lambda h, i: (0, heads + h)),
            pl.BlockSpec((1, VDIM), lambda h, i: (0, 0)),
        ],
        out_specs=pl.BlockSpec((tile, VDIM), lambda h, i: (i, h)),
        out_shape=jax.ShapeDtypeStruct((tok, heads * VDIM), jnp.bfloat16),
        cost_estimate=pl.CostEstimate(
            flops=heads * tok * rows * 2 * 2 * (HEAD + VDIM),
            bytes_accessed=2 * (q.size * 2 + kv.size),
            transcendentals=heads * 2 * tok * rows,
        ),
    )(lam, q, kv, kv, gain.reshape(1, VDIM))


def general_body(
    tokens,
    norm_gain,
    query_diff,
    key_diff,
    value_diff,
    lam,
    output_norm_gain,
    query_win,
    keyval_win,
    sink,
    proj_diff,
    proj_win,
):
    bf16, f32 = jnp.bfloat16, jnp.float32
    normed = root_mean_square_rows(tokens.astype(f32), norm_gain).astype(bf16)
    heads_win = sink.shape[0]
    group = WIN_HEADS // KV_HEADS
    n = lax.axis_size("sp")
    me = lax.axis_index("sp")
    parts = lax.axis_size("grp")
    part = lax.axis_index("grp")
    local, width = normed.shape
    depth = width // n
    tok = local * lax.axis_size("tp")

    slabs = normed.reshape(local, n, depth)
    across = jnp.zeros((n, local, depth), bf16)
    own = lax.dynamic_index_in_dim(slabs, me, 1, keepdims=True)
    across = lax.dynamic_update_slice_in_dim(across, jnp.swapaxes(own, 0, 1), me, 0)
    for r in range(1, n):
        sent = lax.dynamic_index_in_dim(slabs, (me + r) % n, 1, keepdims=False)
        got = shifted(sent, "sp", r)
        across = lax.dynamic_update_slice_in_dim(across, got[None], (me - r) % n, 0)

    kv_index = lax.axis_index("tp") * heads_win // group
    kv_local = lax.dynamic_index_in_dim(keyval_win, kv_index, 0, keepdims=False)
    stacked = jnp.concatenate([query_diff, query_win, kv_local], axis=1)
    share = stacked.shape[1] // parts
    half = lax.dynamic_slice_in_dim(stacked, part * share, share, axis=1)
    across, half = lax.optimization_barrier((across, half))

    pieces = [shifted(half, "sp", r) for r in range(1, n)]
    all_rows = gather_tp(across, 1).reshape(n * tok, depth)
    rows_all = gather_tp(normed, 0).reshape(tok, width)
    kv_part = jnp.concatenate(
        [
            jnp.dot(all_rows, key_diff, preferred_element_type=f32).astype(bf16),
            jnp.dot(all_rows, value_diff, preferred_element_type=f32).astype(bf16),
        ],
        axis=1,
    )
    kv = lax.psum_scatter(kv_part, "sp", scatter_dimension=0, tiled=True)
    kv = lax.all_gather(kv, "sp", axis=0, tiled=True)

    own_rows = lax.dynamic_slice_in_dim(rows_all, me * depth, depth, axis=1)
    own_sum = jnp.dot(own_rows, stacked, preferred_element_type=f32)
    sums = [jnp.zeros((tok, share), f32) for _ in range(parts)]
    for r in range(1, n):
        piece = pieces[r - 1]
        rows = lax.dynamic_slice_in_dim(rows_all, (me - r) % n * depth, depth, axis=1)
        for j in range(parts):
            block = piece if j == 0 else shifted(piece, "grp", j)
            sums[j] = sums[j] + jnp.dot(rows, block, preferred_element_type=f32)
    ordered = jnp.stack(sums)
    ordered = jnp.concatenate(
        [
            lax.dynamic_index_in_dim(ordered, (part - b) % parts, 0, keepdims=False)
            for b in range(parts)
        ],
        axis=1,
    )
    projected = (own_sum + ordered).astype(bf16)
    first = query_diff.shape[1]
    second = first + query_win.shape[1]
    q_diff, q_win, kv_win = projected[:, :first], projected[:, first:second], projected[:, second:]
    scale = HEAD ** (-0.5)
    padded = padded_2(kv_win, (("sp", 0),), WINDOW)
    nblocks = tok // WINDOW
    blocks = padded.reshape(nblocks + 2, WINDOW, 2 * HEAD)
    band = jnp.concatenate([blocks[:-2], blocks[1:-1], blocks[2:]], axis=1)
    q_blocks = q_win.reshape(nblocks, WINDOW, heads_win, HEAD)
    scores = (
        jnp.einsum("nqhd,nkd->nhqk", q_blocks, band[..., :HEAD], preferred_element_type=jnp.float32)
        * scale
    )
    q_index = jnp.arange(WINDOW)
    k_index = jnp.arange(3 * WINDOW)
    relative = k_index[None, :] - WINDOW - q_index[:, None]
    first_key = lax.axis_index("sp") * tok - WINDOW
    key_pos = first_key + jnp.arange(nblocks)[:, None] * WINDOW + k_index[None, :]
    inside = (key_pos >= 0) & (key_pos < tok * lax.axis_size("sp"))
    valid = (jnp.abs(relative) <= WINDOW)[None] & inside[:, None, :]
    scores = jnp.where(valid[:, None], scores, -jnp.inf)
    sink_logit = sink[None, :, None, None]
    top_win = jnp.maximum(jnp.max(scores, axis=-1, keepdims=True), sink_logit)
    expo = jnp.exp(scores - top_win)
    weights = expo / (jnp.sum(expo, axis=-1, keepdims=True) + jnp.exp(sink_logit - top_win))
    y_win = jnp.einsum(
        "nhqk,nkd->nqhd",
        weights.astype(jnp.bfloat16),
        band[..., HEAD:],
        preferred_element_type=jnp.float32,
    ).astype(jnp.bfloat16)
    y_win = y_win.reshape(tok, heads_win * HEAD)
    summed = jnp.dot(y_win, proj_win, preferred_element_type=jnp.float32)
    differential_output = diff_attention(q_diff, kv, lam, output_norm_gain)
    summed = summed + jnp.dot(differential_output, proj_diff, preferred_element_type=jnp.float32)
    return scatter_tp(summed)


MESH = pl.DeviceIdType.MESH
CHUNKS = 4
LANES = 128
MATS = 5


def remote(src, dst, send, recv, device):
    return pltpu.make_async_remote_copy(
        src_ref=src, dst_ref=dst, send_sem=send, recv_sem=recv, device_id=device, device_id_type=MESH
    )


def place():
    g, z, t = lax.axis_index("grp"), lax.axis_index("sp"), lax.axis_index("tp")
    x, c = t // 2, t % 2
    return g, z, t, x, c, 2 * (1 - x) + c, 2 * x + 1 - c


def greet(devices, meanwhile):
    barrier = pltpu.get_barrier_semaphore()
    for device in devices:
        pl.semaphore_signal(barrier, inc=1, device_id=device, device_id_type=MESH)
    meanwhile()
    pl.semaphore_wait(barrier, len(devices))


def arrivals(n, here):
    times = []
    for k in range(1, n):
        for h in range(CHUNKS):
            at = k - 1 + (h + 1) / CHUNKS
            if here - k >= 0:
                times.append((at, "z", here - k, h, 0, k))
            if here + k < n:
                times.append((at + 0.01, "z", here + k, h, 1, k))
    times.sort()
    clock = 0.0
    beside = []
    for at, zz, h in [(0.0, here, h) for h in range(CHUNKS)] + [(e[0], e[2], e[3]) for e in times]:
        clock = max(clock, at) + 1 / CHUNKS
        beside.append((clock + 0.05, "x", zz, h, 0, 0))
    return times + beside


def order(n, here):
    def start(zz):
        return (zz + 1 if zz < here else n - zz, abs(zz - here))

    return sorted((zz for zz in range(n) if zz != here), key=start)


def whole_kernel(
    n, held, tok_hbm, gain_hbm, qd, qw, kd, vd, kvw, pd, pw, lam_ref, sink_ref, out_gain_ref,
    out_ref,
    tok_ref, gain_ref, scal_ref, enter, rows_ref, w_ref, sum_ref, res_ref, oscal_ref, p_ref, v_ref, y_ref, got_ref, mine_ref, away_ref, theirs_ref,
    zs, zr, xs, xr, cs, cr, ws, wr, ys, yr, own_sem, rs, rr, ps, pr, load, scal_s, scal_r, hs, hr, ds, dr,
):
    g, z, t, x, c, t_x, t_c = place()
    local, width = tok_hbm.shape
    part = local // CHUNKS
    depth = qd.shape[0]
    half = depth // 2
    group = WIN_HEADS // KV_HEADS
    mats = (qd, qw, kd, vd, kvw)
    core = (g, z, t_c)
    f32, bf16 = jnp.float32, jnp.bfloat16

    def block(zz, h, tt):
        return rows_ref.at[zz, h, pl.ds(pl.multiple_of(tt * part, part), part)]

    entries = [pltpu.make_async_copy(tok_hbm, tok_ref, enter.at[0]), pltpu.make_async_copy(gain_hbm, gain_ref, enter.at[1])]
    for copy in entries:
        copy.start()

    def normalize():
        scal_ref[...] = jnp.zeros(scal_ref.shape, f32)
        scal_ref[0:1, 0:held] = lam_ref[...]
        scal_ref[1:2, 0:2 * held] = sink_ref[...]
        oscal_ref[c] = scal_ref[...]
        for copy in entries:
            copy.wait()
        for h in range(CHUNKS):
            v = tok_ref[h * part:(h + 1) * part, :].astype(f32)
            v = v * lax.rsqrt(jnp.mean(v * v, axis=-1, keepdims=True) + EPS) * gain_ref[...]
            rows_ref[z, h, pl.ds(pl.multiple_of(t * part, part), part), :] = v.astype(bf16)

    greet(
        [(g, lax.rem(z + i // 2, n), 2 * x + (c + i % 2) % 2) for i in range(1, 2 * n)]
        + [(g, z, t_x), (1 - g, z, t)],
        normalize,
    )

    def w_half(zz, yy, m):
        at = pl.ds(pl.multiple_of(zz * depth + yy * half, half), half)
        return w_ref.at[at, m * LANES:(m + 1) * LANES]

    def source(dz, i, cc, m, at):
        if m == MATS - 1:
            return kvw.at[(2 * (x * n + dz)) // group, at, cc * LANES:(cc + 1) * LANES]
        return mats[m].at[at, (2 * i + cc) * LANES:(2 * i + cc + 1) * LANES]

    def w_copy(here, dz, cc, m):
        at = pl.ds(pl.multiple_of(g * half, half), half)
        return remote(
            source(dz, dz % held, cc, m, at), w_half(here, g, m),
            ws.at[dz % held, cc, m], wr.at[here, m], (g, dz, 2 * x + cc),
        )

    def w_each(here, way, act):
        for cs_ in range(2):
            @pl.when(c == cs_)
            def _():
                for m in range(MATS):
                    for dz in sorted(range(cs_ * held, (cs_ + 1) * held), key=lambda o: abs(o - here)):
                        if (dz > here) if way == 0 else (dz < here):
                            for cc in range(2):
                                act(w_copy(here, dz, cc, m))

    def own_copy(here, cc, m):
        at = pl.ds(0, depth)
        target = w_ref.at[here * depth:(here + 1) * depth, m * LANES:(m + 1) * LANES]
        return source(here, here % held, cc, m, at), target

    def own_each(here, near, away):
        for cc in range(2):
            for m in range(MATS):
                a, b = own_copy(here, cc, m)

                if near is not None:
                    @pl.when((c == here // held) & (c == cc))
                    def _():
                        near(pltpu.make_async_copy(a, b, own_sem.at[m]))

                @pl.when((c == here // held) & (c != cc))
                def _():
                    away(remote(a, b, ws.at[here % held, cc, m], own_sem.at[m], core))

    def z_copy(zz, h, way, here):
        k = abs(zz - here)
        to = here + 1 if way == 0 else here - 1
        return remote(block(zz, h, t), block(zz, h, t), zs.at[way, k, h], zr.at[way, k + 1, h], (g, to, t))

    def x_copy(zz, h):
        return remote(block(zz, h, t), block(zz, h, t), xs.at[zz, h], xr.at[zz, h], (g, z, t_x))

    def c_copy(zz, xx, h):
        tt = 2 * xx + c
        return remote(block(zz, h, tt), block(zz, h, tt), cs.at[zz, xx, h], cr.at[zz, xx, h], core)

    def y_copy(zz, m):
        return remote(w_half(zz, g, m), w_half(zz, g, m), ys.at[zz, m], yr.at[zz, m], (1 - g, z, t))

    def forward(zz, m):
        remote(w_half(zz, g, m), w_half(zz, g, m), ys.at[zz, m], wr.at[zz, m], core).wait_recv()
        y_copy(zz, m).start()

    def crossed(zz):
        for m in range(MATS):
            remote(w_half(zz, 1 - g, m), w_half(zz, 1 - g, m), ys.at[zz, m], yr.at[zz, m], core).wait_recv()

    scal_copy = remote(scal_ref, oscal_ref.at[c], scal_s, scal_r, core)

    proj_copies, loads = [], []
    for i in range(held):
        for j, ref in enumerate((pd, pw)):
            rows = ref.at[i * VDIM:(i + 1) * VDIM]
            at = p_ref.at[c * held + i, j * VDIM:(j + 1) * VDIM]
            loads.append(pltpu.make_async_copy(rows, at, load.at[i, j]))
            proj_copies.append(remote(rows, at, ps.at[i, j], pr.at[i, j], core))

    def gather(here):
        for h in range(CHUNKS):
            if here < n - 1:
                z_copy(here, h, 0, here).start()
            if here > 0:
                z_copy(here, h, 1, here).start()
            x_copy(here, h).start()
            c_copy(here, x, h).start()
        scal_copy.start()
        for copy in loads + proj_copies:
            copy.start()
        own_each(here, lambda copy: copy.start(), lambda copy: copy.start())
        if here == 0:
            w_each(here, 0, lambda copy: copy.start())
        if here == n - 1:
            w_each(here, 1, lambda copy: copy.start())
        first = order(n, here)[0]
        begin = first + 1 if first < here else n - first
        events = arrivals(n, here)
        events += [(begin + 0.5 * (m + 1), "w", first, m, 0, 0) for m in range(MATS)]
        for at, kind, zz, h, way, k in sorted(events):
            if kind == "z":
                remote(block(zz, h, t), block(zz, h, t), zs.at[way, k, h], zr.at[way, k, h], core).wait_recv()
                if (here < n - 1) if way == 0 else (here > 0):
                    z_copy(zz, h, way, here).start()
                x_copy(zz, h).start()
                c_copy(zz, x, h).start()
                if h == CHUNKS - 1 and zz == (0 if way == 0 else n - 1):
                    w_each(here, way, lambda copy: copy.start())
            elif kind == "x":
                x_copy(zz, h).wait_recv()
                c_copy(zz, 1 - x, h).start()
            else:
                forward(zz, h)

    for here in range(n):
        pl.when(z == here)(functools.partial(gather, here))


    sources = []
    for j in range(n - 1):
        zz = order(n, 0)[j] + 0 * z
        for here in range(1, n):
            zz = jnp.where(z == here, order(n, here)[j], zz)
        sources.append(zz)

    quad = rows_ref.shape[2]

    def partial_sum(zz, at, size):
        k = pl.ds(pl.multiple_of(at, half), size)
        left = rows_ref[zz, :, :, k].reshape(CHUNKS * quad, size)
        return jnp.dot(left, w_ref[k, :], preferred_element_type=f32)

    def opening(zz, carry):
        for xx in range(2):
            for h in range(CHUNKS):
                c_copy(zz, xx, h).wait_recv()
        sum_ref[zz] = partial_sum(zz, z * depth, depth)
        return carry

    def add(at):
        def one(zz, carry):
            sum_ref[zz] += partial_sum(zz, at, half)
            return carry

        lax.fori_loop(0, n, one, 0)

    def r_copies(zz):
        copies = [remote(
            res_ref.at[c, zz, :, :, 2 * LANES:], res_ref.at[c, zz, :, :, 2 * LANES:],
            rs.at[zz, 0], rr.at[zz, 0], core,
        )]
        for xx in range(2):
            at = pl.ds(pl.multiple_of((2 * xx + 1 - c) * part, part), part)
            copies.append(remote(
                res_ref.at[c, zz, :, at, :2 * LANES], res_ref.at[c, zz, :, at, :2 * LANES],
                rs.at[zz, 1 + xx], rr.at[zz, 1 + xx], core,
            ))
        return copies

    for m in range(MATS):
        a, b = own_copy(0, 0, m)
        pltpu.make_async_copy(a, b, own_sem.at[m]).wait()
    late = sources[1:]

    def forwards(lo, hi):
        for m in range(lo, hi):
            for zz in late:
                forward(zz, m)

    forwards(0, 2)
    lax.fori_loop(0, n, opening, 0)
    forwards(2, 3)
    add(sources[0] * depth + g * half)
    crossed(sources[0])
    add(sources[0] * depth + (1 - g) * half)
    forwards(3, MATS)
    for zz in late:
        add(zz * depth + g * half)
    for zz in late[:-1]:
        crossed(zz)
        add(zz * depth + (1 - g) * half)
    crossed(sources[-1])

    def closing(zz, carry):
        total = sum_ref[zz] + partial_sum(zz, sources[-1] * depth + (1 - g) * half, half)

        @pl.when(zz > 0)
        def _():
            for copy in r_copies(zz - 1):
                copy.start()

        res_ref[c, zz] = total.astype(bf16).reshape(CHUNKS, quad, MATS * LANES)
        return carry

    lax.fori_loop(0, n, closing, 0)
    scal_copy.wait()
    for copy in r_copies(n - 1):
        copy.start()

    def exchanged(zz, carry):
        for copy in r_copies(zz):
            copy.wait_recv()
        return carry

    lax.fori_loop(0, n, exchanged, 0)

    rows = n * 4 * local
    factor = HEAD ** (-0.5) * math.log2(math.e)
    for i in range(2):
        v_ref[:, i * LANES:(i + 1) * LANES] = res_ref[i, :, :, :, 3 * LANES:4 * LANES].reshape(rows, LANES)

    level = oscal_ref[z // held]
    level_row = lax.broadcasted_iota(jnp.int32, level.shape, 0)
    level_lane = lax.broadcasted_iota(jnp.int32, level.shape, 1)

    def scalar(row, lane):
        picked = jnp.where((level_row == row) & (level_lane == lane), level, 0.0)
        return jnp.sum(jnp.sum(picked, axis=1, keepdims=True), axis=0, keepdims=True)

    lam = scalar(0, z % held)
    sinks = [scalar(1, 2 * (z % held) + i) for i in range(2)]
    first = lax.broadcasted_iota(jnp.int32, (local, 1), 0) < local // 2
    sink = jnp.where(first, sinks[0], sinks[1])

    distant = []
    for j in range(n):
        zz = 0 * z
        for here in range(n):
            far = sorted(range(n), key=lambda o: -abs(o - here))[j]
            zz = jnp.where(z == here, far, zz)
        distant.append(zz)

    fine = local // 2
    some = CHUNKS // 2

    def piece(i, zz, tt, m, e=None):
        at = pl.ds(pl.multiple_of(tt * part, part), part)
        if e is None:
            return res_ref[i, zz, :, at, m * LANES:(m + 1) * LANES].reshape(local, LANES)
        return res_ref[i, zz, pl.ds(e * some, some), at, m * LANES:(m + 1) * LANES].reshape(fine, LANES)

    def rows_of(e):
        return pl.ds(pl.multiple_of(e * fine, fine), fine)

    def y_copy_to(zz, xx, e):
        return remote(
            y_ref.at[zz, xx, rows_of(e)], got_ref.at[z, xx, rows_of(e)],
            hs.at[zz, xx, e], hr.at[z, xx, e], (g, zz, t),
        )

    def y_wait(zz, xx, e):
        rows = got_ref.at[zz, xx, rows_of(e)]
        return remote(rows, rows, hs.at[zz, xx, e], hr.at[zz, xx, e], (g, z, t_x))

    def windowed(zz, tt, xx, e):
        b = 4 * zz + tt

        def banded(i):
            pieces = []
            for o in (-1, 0, 1):
                o = jnp.clip(b + o, 0, 4 * n - 1)
                pieces.append(piece(i, o // 4, o % 4, 4))
            return jnp.concatenate(pieces, axis=0)

        q = jnp.concatenate([piece(i, zz, tt, 1, e) for i in range(2)], axis=0)
        scores = lax.dot_general(
            q, banded(0), (((1,), (1,)), ((), ())), preferred_element_type=f32
        ) * HEAD ** (-0.5)
        r_index = lax.broadcasted_iota(jnp.int32, scores.shape, 0) % fine + e * fine
        k_index = lax.broadcasted_iota(jnp.int32, scores.shape, 1)
        spot = (b - 1) * local + k_index
        valid = (jnp.abs(k_index - local - r_index) <= WINDOW) & (spot >= 0) & (spot < rows)
        scores = jnp.where(valid, scores, -jnp.inf)
        top = jnp.maximum(jnp.max(scores, axis=-1, keepdims=True), sink)
        expo = jnp.exp(scores - top)
        weights = expo / (jnp.sum(expo, axis=-1, keepdims=True) + jnp.exp(sink - top))
        out = jnp.dot(weights.astype(bf16), banded(1), preferred_element_type=f32).astype(bf16)
        for i in range(2):
            y_ref[zz, xx, rows_of(e), VDIM + i * LANES:VDIM + (i + 1) * LANES] = out[i * fine:(i + 1) * fine]

    def attend(step):
        xx = jnp.where(step < 2, 1 - x, x)
        tt = 2 * xx + c
        e = step % 2
        maps = []
        for m in range(2):
            q = jnp.concatenate([piece(m, zz, tt, 0, e) for zz in distant], axis=0)
            keys = res_ref[m, :, :, :, 2 * LANES:3 * LANES].reshape(rows, LANES)
            scores = lax.dot_general(q, keys, (((1,), (1,)), ((), ())), preferred_element_type=f32)
            top = jnp.max(scores, axis=-1, keepdims=True)
            expo = jnp.exp2((scores - top) * factor)
            total = jnp.sum(expo, axis=-1, keepdims=True)
            out = jnp.dot(expo.astype(bf16), v_ref[...], preferred_element_type=f32)
            maps.append(out / total)
        d = maps[0] - lam * maps[1]
        d = d * lax.rsqrt(jnp.mean(d * d, axis=-1, keepdims=True) + EPS) * out_gain_ref[...]
        d = d.astype(bf16)
        for i, zz in enumerate(distant):
            y_ref[zz, xx, rows_of(e), :VDIM] = d[i * fine:(i + 1) * fine]
        for zz in distant:
            windowed(zz, tt, xx, e)
        for zz in distant:
            @pl.when(zz != z)
            def _():
                y_copy_to(zz, xx, e).start()
        got_ref[z, xx, rows_of(e)] = y_ref[z, xx, rows_of(e)]

    steps = mine_ref.shape[1]
    wide = width // steps

    def others(act):
        for d in range(n - 1, 0, -1):
            pl.when(z - d >= 0)(functools.partial(act, z - d))
            pl.when(z + d < n)(functools.partial(act, z + d))

    def product(j, xx, e):
        total = jnp.zeros((fine, wide), f32)
        at = pl.ds(pl.multiple_of(j * wide, wide), wide)
        for zz in range(n):
            total = total + jnp.dot(
                got_ref[zz, xx, rows_of(e)], p_ref[zz, :, at], preferred_element_type=f32
            )
        return total

    def d_copy(e, j):
        return remote(away_ref.at[e, j], theirs_ref.at[e, j], ds.at[e, j], dr.at[e, j], (g, z, t_x))

    def send_rows(e):
        @pl.when(e == 0)
        def _():
            for copy in loads + proj_copies:
                copy.wait()

        others(lambda zz: y_wait(zz, 1 - x, e).wait_recv())

        def send(j, carry):
            value = product(j, 1 - x, e).astype(bf16)

            @pl.when(j > 0)
            def _():
                d_copy(e, j - 1).start()

            away_ref[e, j] = value
            return carry

        lax.fori_loop(0, steps, send, 0)
        d_copy(e, steps - 1).start()

    def stage(step, carry):
        attend(step)
        pl.when((step >= 1) & (step <= 2))(lambda: send_rows(step - 1))
        return carry

    lax.fori_loop(0, 4, stage, 0)

    def keep_rows(e, carry):
        others(lambda zz: y_wait(zz, x, e).wait_recv())

        def keep(j, carry):
            mine_ref[e, j] = product(j, x, e)
            return carry

        lax.fori_loop(0, steps, keep, 0)
        return carry

    lax.fori_loop(0, 2, keep_rows, 0)
    for e in range(2):
        for j in range(steps):
            d_copy(e, j).wait_recv()
            total = mine_ref[e, j] + theirs_ref[e, j].astype(f32)
            out_ref[e * fine:(e + 1) * fine, j * wide:(j + 1) * wide] = total.astype(bf16)
    for e in range(2):
        for j in range(steps):
            d_copy(e, j).wait_send()
        for xx in (1 - x, x):
            others(lambda zz: y_copy_to(zz, xx, e).wait_send())

    def drain(here):
        for way in range(2):
            if (here < n - 1) if way == 0 else (here > 0):
                w_each(here, way, lambda copy: copy.wait_send())
                for zz in (range(here + 1) if way == 0 else range(here, n)):
                    for h in range(CHUNKS):
                        z_copy(zz, h, way, here).wait_send()
        own_each(here, None, lambda copy: copy.wait_send())

    for here in range(n):
        pl.when(z == here)(functools.partial(drain, here))

    def finished(zz, carry):
        for h in range(CHUNKS):
            x_copy(zz, h).wait_send()
            for xx in range(2):
                c_copy(zz, xx, h).wait_send()

        @pl.when(zz != z)
        def _():
            for m in range(MATS):
                y_copy(zz, m).wait_send()

        for copy in r_copies(zz):
            copy.wait_send()
        return carry

    lax.fori_loop(0, n, finished, 0)


def whole(
    n, tokens, norm_gain, query_diff, query_win, key_diff, value_diff, keyval_win, proj_diff, proj_win, lam, sink,
    output_norm_gain,
):
    local, width = tokens.shape
    held = n // 2
    dma = pltpu.SemaphoreType.DMA
    inside = pl.BlockSpec(memory_space=pltpu.VMEM)
    far = pl.BlockSpec(memory_space=pl.ANY)
    cols = MATS * LANES
    tok = 4 * local * n
    feats = VDIM + 2 * HEAD
    steps = 4
    quad = 4 * local // CHUNKS
    bf16, f32 = jnp.bfloat16, jnp.float32
    return pl.pallas_call(
        functools.partial(whole_kernel, n, held),
        in_specs=[far] * 9 + [inside] * 3,
        out_specs=inside,
        out_shape=jax.ShapeDtypeStruct((local, width), bf16),
        scratch_shapes=[
            pltpu.VMEM((local, width), bf16),
            pltpu.VMEM((1, width), f32),
            pltpu.VMEM((8, LANES), f32),
            dma((2,)),
            pltpu.VMEM((n, CHUNKS, quad, width), bf16),
            pltpu.VMEM((width, cols), bf16),
            pltpu.VMEM((n, 4 * local, cols), f32),
            pltpu.VMEM((2, n, CHUNKS, quad, cols), bf16),
            pltpu.VMEM((2, 8, LANES), f32),
            pltpu.VMEM((n, feats, width), bf16),
            pltpu.VMEM((tok, VDIM), bf16),
            pltpu.VMEM((n, 2, local, feats), bf16),
            pltpu.VMEM((n, 2, local, feats), bf16),
            pltpu.VMEM((2, steps, local // 2, width // steps), f32),
            pltpu.VMEM((2, steps, local // 2, width // steps), bf16),
            pltpu.VMEM((2, steps, local // 2, width // steps), bf16),
            dma((2, n, CHUNKS)), dma((2, n + 1, CHUNKS)),
            dma((n, CHUNKS)), dma((n, CHUNKS)),
            dma((n, 2, CHUNKS)), dma((n, 2, CHUNKS)),
            dma((held, 2, MATS)), dma((n, MATS)),
            dma((n, MATS)), dma((n, MATS)), dma((MATS,)),
            dma((n, 3)), dma((n, 3)),
            dma((held, 2)), dma((held, 2)), dma((held, 2)), dma, dma,
            dma((n, 2, 2)), dma((n, 2, 2)), dma((2, steps)), dma((2, steps)),
        ],
        compiler_params=pltpu.CompilerParams(
            collective_id=0, has_side_effects=True, vmem_limit_bytes=67043328
        ),
        cost_estimate=pl.CostEstimate(
            flops=2 * tok * width * cols, bytes_accessed=2 * width * (tok + cols), transcendentals=0
        ),
    )(
        tokens, norm_gain.reshape(1, width), query_diff, query_win, key_diff, value_diff, keyval_win,
        proj_diff, proj_win, lam.reshape(1, -1), sink.reshape(1, -1), output_norm_gain.reshape(1, VDIM),
    )


def split_body(
    tokens, norm_gain, query_diff, key_diff, value_diff, lam, output_norm_gain,
    query_win, keyval_win, sink, proj_diff, proj_win,
):
    n = lax.axis_size("sp")
    return whole(
        n, tokens, norm_gain, query_diff, query_win, key_diff, value_diff, keyval_win, proj_diff, proj_win, lam, sink,
        output_norm_gain,
    )


def splits(mesh, tokens, query_diff, query_win, lam, sink):
    parts, n, tp = (mesh.shape[a] for a in ("grp", "sp", "tp"))
    return (
        parts == 2 and tp == 4 and n % 2 == 0
        and lam.shape[0] == 2 * n and sink.shape[0] == 2 * lam.shape[0]
        and tokens.shape[0] == parts * n * tp * WINDOW
        and query_diff.shape[1] == lam.shape[0] * 2 * HEAD and VDIM == 2 * HEAD
        and query_win.shape[1] == sink.shape[0] * HEAD and HEAD == LANES
    )


def solution(mesh):
    placed = (
        P(("grp", "sp", "tp"), None),
        P(),
        P("sp", "tp"),
        P("sp", "tp"),
        P("sp", "tp"),
        P("tp"),
        P(),
        P("sp", "tp"),
        P(None, "sp", None),
        P("tp"),
        P("tp", None),
        P("tp", None),
    )

    def build(body):
        return jax.shard_map(
            body, mesh=mesh, in_specs=placed, out_specs=P(("grp", "sp", "tp"), None), check_vma=False
        )

    general = build(general_body)

    def step(*args):
        tokens, query_diff, lam, query_win, sink = (args[i] for i in (0, 2, 5, 7, 9))
        if splits(mesh, tokens, query_diff, query_win, lam, sink):
            return build(split_body)(*args)
        return general(*args)

    return step
```
